32 devices in a mesh: sp: 8 (over z, x), tp: 4 (over y, core).
Axes of the slice: x: 2, y: 2, z: 4, core: 2. Of those that a mesh axis runs over, the one named last changes fastest.
Arguments:
- tokens: bfloat16 [3072, 2048], P('sp', 'tp'), may hold values from -6 to 6
- pre_gain: float32 [2048], replicated, may hold values from 0.1 to 1.9
- outer_gate_weight: bfloat16 [2048, 1024], P(None, 'tp'), may hold values from -0.125 to 0.125
- inner_gate_weight: bfloat16 [2048, 1024], P(None, 'tp'), may hold values from -0.125 to 0.125
- source_weight: bfloat16 [2048, 1024], P(None, 'tp'), may hold values from -0.125 to 0.125
- conv_taps: bfloat16 [3, 1024], P(None, 'tp'), may hold values from -3.5 to 3.5
- q_down_weight: bfloat16 [2048, 768], replicated, may hold values from -0.125 to 0.125
- q_norm_gain: float32 [768], replicated, may hold values from 0.5 to 16
- q_up_weight: bfloat16 [768, 3072], P(None, 'tp'), may hold values from -0.21875 to 0.21875
- kv_down_weight: bfloat16 [2048, 512], replicated, may hold values from -0.125 to 0.125
- rope_key_weight: bfloat16 [2048, 32], replicated, may hold values from -0.125 to 0.125
- kv_norm_gain: float32 [512], replicated, may hold values from 0.5 to 16
- kv_up_weight: bfloat16 [512, 4096], P(None, 'tp'), may hold values from -0.25 to 0.25
- attn_out_weight: bfloat16 [2048, 2048], P('tp'), may hold values from -4 to 4
- conv_out_weight: bfloat16 [1024, 2048], P('tp'), may hold values from -0.1875 to 0.1875
- post_gain: float32 [2048], P('tp'), may hold values from 0.1 to 1.9
Outputs:
- mixed: bfloat16 [3072, 2048], P('sp', 'tp')
- log_total: float32 [32, 3072], P('tp', 'sp')
The draws below stay inside these ranges and needn't reach their ends.
All inputs are finite; a program needn't handle non-finite values.
Results may differ from the reference program's by a relative error of at most 0.017.
The reference program's roundings to bfloat16 on the way count: a program that leaves them out, or rounds other values in their place, can miss the bound.
Values may be sent and summed in bfloat16 or wider, within the bound.
A program may use at most 128 MiB of HBM per device.

```python
import jax
import jax.numpy as jnp
from jax import lax

D = 2048
HEADS = 32
NOPE = 64
ROPE = 32
VDIM = 64
Q_RANK = 768
KV_RANK = 512
CONV_W = 1024
TAPS = 3
TOK_DEV = 384
TOKENS = 3072
N_SP = 8
N_TP = 4


def latent_gain(key, count):
    upper = 2.0
    return jnp.exp(jax.random.uniform(key, (count,), jnp.float32, jnp.log(0.5), jnp.log(upper)))


def draw_q_norm_gain(key, part):
    return latent_gain(jax.random.fold_in(key, 11), Q_RANK)


def draw_kv_norm_gain(key, part):
    return latent_gain(jax.random.fold_in(key, 23), KV_RANK)


def block_levels(stream_key, shape, shards, low, high):
    gain, own = 1.0, jax.random.fold_in(stream_key, 6)
    for dim, parts in shards:
        steps = jnp.exp(jax.random.uniform(jax.random.fold_in(own, dim), (parts,), jnp.float32, low / len(shards), high / len(shards)))
        gain = gain * jnp.repeat(steps, shape[dim] // parts).reshape([-1 if axis == dim else 1 for axis in range(len(shape))])
    return gain


def centred(stream_key, dims, scale, bound, split=(), held_as=jnp.bfloat16):
    values = scale * jax.random.normal(stream_key, dims, jnp.float32)
    if split:
        values = values * block_levels(stream_key, dims, split, -0.22, 0.18)
    return jnp.clip(values, -bound, bound).astype(held_as)


def setup_inputs(seed: int = 0) -> dict:
    splits = jax.random.split(jax.random.key(seed), 17)
    return {
        "tokens": centred(splits[0], (TOKENS, D), 1.0, 6.0, ((0, 8), (1, 4))),
        "pre_gain": jnp.clip(1.0 + 0.18 * jax.random.normal(splits[1], (D,), jnp.float32), 0.1, 1.9),
        "outer_gate_weight": centred(splits[2], (D, CONV_W), D ** -0.5, 0.125, ((1, 4),)),
        "inner_gate_weight": centred(splits[3], (D, CONV_W), D ** -0.5, 0.125, ((1, 4),)),
        "source_weight": centred(splits[4], (D, CONV_W), D ** -0.5, 0.125, ((1, 4),)),
        "conv_taps": centred(splits[5], (TAPS, CONV_W), TAPS ** -0.5, 3.5, ((1, 4),)),
        "q_down_weight": centred(splits[6], (D, Q_RANK), D ** -0.5, 0.125),
        "q_norm_gain": draw_q_norm_gain(jax.random.fold_in(splits[16], 71), 0),
        "q_up_weight": centred(splits[8], (Q_RANK, HEADS * (NOPE + ROPE)), Q_RANK ** -0.5, 0.21875, ((1, 4),)),
        "kv_down_weight": centred(splits[9], (D, KV_RANK), D ** -0.5, 0.125),
        "rope_key_weight": centred(splits[10], (D, ROPE), D ** -0.5, 0.125),
        "kv_norm_gain": draw_kv_norm_gain(jax.random.fold_in(splits[16], 71), 0),
        "kv_up_weight": centred(splits[12], (KV_RANK, HEADS * (NOPE + VDIM)), KV_RANK ** -0.5, 0.25, ((1, 4),)),
        "attn_out_weight": centred(splits[13], (HEADS * VDIM, D), 2 ** -0.5, 4.0, ((0, 4),)),
        "conv_out_weight": centred(splits[14], (CONV_W, D), CONV_W ** -0.5, 0.1875, ((0, 4),)),
        "post_gain": jnp.clip(1.0 + 0.18 * jax.random.normal(splits[15], (D,), jnp.float32), 0.1, 1.9),
    }


EPSILON = 1e-06
THETA = 500000.0

def rms_scale(values):
    return lax.rsqrt(lax.optimization_barrier(jnp.mean(values * values, axis=-1, keepdims=True)) + EPSILON)

def rotation(positions, width):
    freqs = THETA ** (-jnp.arange(0, width, 2, dtype=jnp.float32) / width)
    angles = positions.astype(jnp.float32)[:, None] * freqs[None, :]
    return (jnp.cos(angles), jnp.sin(angles))

def rotate(values, cosine, sine):
    half = values.shape[-1] // 2
    first = values[..., :half]
    second = values[..., half:]
    return jnp.concatenate([first * cosine - second * sine, second * cosine + first * sine], axis=-1)

def reference(tokens, pre_gain, outer_gate_weight, inner_gate_weight, source_weight, conv_taps, q_down_weight, q_norm_gain, q_up_weight, kv_down_weight, rope_key_weight, kv_norm_gain, kv_up_weight, attn_out_weight, conv_out_weight, post_gain):
    wide = tokens.astype(jnp.float32)
    scaled = (wide * pre_gain).astype(jnp.bfloat16)
    factor = rms_scale(wide)

    def project(weight):
        return jnp.dot(scaled, weight, preferred_element_type=jnp.float32) * factor
    outer = project(outer_gate_weight).astype(jnp.bfloat16)
    inner = project(inner_gate_weight).astype(jnp.bfloat16)
    source = project(source_weight).astype(jnp.bfloat16)
    driven = (inner.astype(jnp.float32) * source.astype(jnp.float32)).astype(jnp.bfloat16)
    padded = jnp.concatenate([jnp.zeros((TAPS - 1, CONV_W), jnp.bfloat16), driven], axis=0)
    convolved = jnp.zeros((TOKENS, CONV_W), jnp.float32)
    for index in range(TAPS):
        convolved = convolved + conv_taps[index].astype(jnp.float32) * padded[index:index + TOKENS].astype(jnp.float32)
    conv_branch = (outer.astype(jnp.float32) * convolved).astype(jnp.bfloat16)
    positions = jnp.arange(TOKENS, dtype=jnp.int32)
    cosine, sine = rotation(positions, ROPE)
    q_latent = project(q_down_weight)
    q_normed = (q_latent * rms_scale(q_latent) * q_norm_gain).astype(jnp.bfloat16)
    query = jnp.dot(q_normed, q_up_weight, preferred_element_type=jnp.float32).reshape(TOKENS, HEADS, NOPE + ROPE)
    q_plain = query[..., :NOPE].astype(jnp.bfloat16)
    q_turned = rotate(query[..., NOPE:], cosine[:, None], sine[:, None]).astype(jnp.bfloat16)
    kv_latent = project(kv_down_weight)
    latent = (kv_latent * rms_scale(kv_latent) * kv_norm_gain).astype(jnp.bfloat16)
    rope_key = rotate(project(rope_key_weight), cosine, sine).astype(jnp.bfloat16)
    keyvals = jnp.dot(latent, kv_up_weight, preferred_element_type=jnp.float32).astype(jnp.bfloat16)
    keyvals = keyvals.reshape(TOKENS, HEADS, NOPE + VDIM)
    head_plain = jnp.transpose(q_plain, (1, 0, 2))
    head_turned = jnp.transpose(q_turned, (1, 0, 2))
    head_keys = jnp.transpose(keyvals[..., :NOPE], (1, 0, 2))
    head_values = jnp.transpose(keyvals[..., NOPE:], (1, 0, 2))
    scale = (NOPE + ROPE) ** (-0.5)
    outputs = []
    logs = []
    for block in range(N_SP):
        first = block * TOK_DEV
        last = first + TOK_DEV
        key_turned = rope_key[:last]
        query_pos = jnp.arange(first, last, dtype=jnp.int32)
        key_pos = jnp.arange(last, dtype=jnp.int32)
        allowed = key_pos[None, :] <= query_pos[:, None]

        def per_head(items):
            plain, turned, keys, values = items
            scores = jnp.dot(plain, keys.T, preferred_element_type=jnp.float32)
            scores = scores + jnp.dot(turned, key_turned.T, preferred_element_type=jnp.float32)
            scores = jnp.where(allowed, scores * scale, -jnp.inf)
            maxima = lax.optimization_barrier(jnp.max(scores, axis=-1, keepdims=True))
            weights = jnp.exp(scores - maxima)
            totals = lax.optimization_barrier(jnp.sum(weights, axis=-1))
            result = jnp.dot(weights.astype(jnp.bfloat16), values, preferred_element_type=jnp.float32) / totals[:, None]
            return (result.astype(jnp.bfloat16), maxima[:, 0] + jnp.log(totals))
        block_out, block_log = lax.map(per_head, (head_plain[:, first:last], head_turned[:, first:last], head_keys[:, :last], head_values[:, :last]))
        outputs.append(block_out)
        logs.append(block_log)
    attended = jnp.concatenate(outputs, axis=1)
    log_total = jnp.concatenate(logs, axis=1)
    attended = jnp.transpose(attended, (1, 0, 2)).reshape(TOKENS, HEADS * VDIM)
    head_rows = HEADS // N_TP * VDIM
    channel_rows = CONV_W // N_TP
    projected = jnp.zeros((TOKENS, D), jnp.float32)
    for group in range(N_TP):
        head_part = jnp.dot(attended[:, group * head_rows:(group + 1) * head_rows], attn_out_weight[group * head_rows:(group + 1) * head_rows], preferred_element_type=jnp.float32)
        conv_part = jnp.dot(conv_branch[:, group * channel_rows:(group + 1) * channel_rows], conv_out_weight[group * channel_rows:(group + 1) * channel_rows], preferred_element_type=jnp.float32)
        rounded = lax.optimization_barrier((head_part + conv_part).astype(jnp.bfloat16))
        projected = projected + rounded.astype(jnp.float32)
    mixed = (projected * rms_scale(projected) * post_gain).astype(jnp.bfloat16)
    return (mixed, log_total)
```

```python
import functools
import math

import jax
import jax.numpy as jnp
import numpy as np
from jax import lax
from jax.experimental import pallas as pl
from jax.experimental.pallas import tpu as pltpu
from jax.sharding import PartitionSpec as P

NOPE = 64
ROPE = 32
VDIM = 64
TAPS = 3
LANES = 128
HALO = 16
TURN = 8
AHEAD = 2
WAVE = 2

EPSILON = 1e-06
THETA = 500000.0
NEGATIVE = -1e30
MESH = pl.DeviceIdType.MESH
BF = jnp.bfloat16
F32 = jnp.float32


def remote(src, dst, send, recv, **where):
    return pltpu.make_async_remote_copy(
        src_ref=src, dst_ref=dst, send_sem=send, recv_sem=recv, device_id=where, device_id_type=MESH
    )


def dot(a, b):
    return jnp.dot(a, b, preferred_element_type=F32)


def dot_nt(a, b):
    return lax.dot_general(a, b, (((1,), (1,)), ((), ())), preferred_element_type=F32)


def layer_kernel(
    nz, nx, n, chunk, heads,
    tok, pre, qg, kg, gain, taps, table, wo, wi, ws, wq, wk, wr, wu, wkv, wa, wc,
    out, logs,
    buf, vo, vi, vs, vq, vk, vr, vu, vkv, va, vc, angle,
    vut, upk, upvt, qt, kvs, kn, turn, vt, sbuf, acc, top, low,
    outer, ext, tail, halo, att,
    away, mine, pin, ysend, yin, peer, pown, total, sq, sqin,
    t_s, w_s, own_s, own_r, y_s, y_r, f_s, f_r,
    z_s, o_s, x_s, i_r, d_s, d_r, h_s, h_r,
    a_s, a_r, b_s, b_r, p_s, p_r, q_s, q_r,
):
    sp, tp = lax.axis_index("sp"), lax.axis_index("tp")
    nsp = nz * nx
    z, x = sp // nx, lax.rem(sp, nx)
    ny = n // 2
    y, core = tp // 2, lax.rem(tp, 2)
    partner = tp + 1 - 2 * core
    rows, width = tok.shape
    count = rows // chunk
    pairs = heads // 2
    rank = wkv.shape[0]
    factor2 = (NOPE + ROPE) ** (-0.5) * math.log2(math.e)
    side = pl.ds(pl.multiple_of(core * (rank // 2), LANES), rank // 2)

    def part(r):
        return pl.ds(r * chunk, chunk)

    tokens = [
        pltpu.make_async_copy(tok.at[part(r)], buf.at[tp, part(r)], t_s.at[r]) for r in range(count)
    ]
    place = pl.ds(pl.multiple_of(sp * rows, LANES), rows)
    pairs_of = (
        (wu, vu), (wkv, vkv), (table.at[:, place], angle), (wk, vk), (wr, vr), (wq, vq),
        (wi, vi), (ws, vs), (wo, vo), (wa, va), (wc, vc),
    )
    loads = [pltpu.make_async_copy(a, b, w_s.at[i]) for i, (a, b) in enumerate(pairs_of)]
    for token in tokens:
        token.start()

    barrier = pltpu.get_barrier_semaphore()

    def greet(**where):
        pl.semaphore_signal(barrier, inc=1, device_id=where, device_id_type=MESH)

    for step in range(1, n):
        greet(tp=lax.rem(tp + step, n))
    for step in range(1, nz):
        greet(sp=lax.rem(z + step, nz) * nx + x)
    for step in range(1, nx):
        greet(sp=z * nx + lax.rem(x + step, nx))
    greet(sp=lax.rem(sp + 1, nsp))
    greet(sp=lax.rem(sp + nsp - 1, nsp))
    for load in loads:
        load.start()
    pl.semaphore_wait(barrier, n - 1 + nz - 1 + nx - 1 + 2)

    def y_copy(r, step):
        to = lax.rem(y + step, ny) * 2 + core
        here = buf.at[tp, part(r)]
        return remote(here, here, y_s.at[r, step], y_r.at[r, y], tp=to)

    def y_arrival(r, other):
        here = buf.at[other * 2 + core, part(r)]
        return remote(here, here, y_s.at[r, 0], y_r.at[r, other], tp=partner)

    def own_copy(r):
        here = buf.at[tp, part(r)]
        return remote(here, here, own_s.at[r], own_r.at[r], tp=partner)

    def own_arrival(r):
        here = buf.at[partner, part(r)]
        return remote(here, here, own_s.at[r], own_r.at[r], tp=partner)

    def forward(r, other):
        here = buf.at[other * 2 + core, part(r)]
        return remote(here, here, f_s.at[r, other], f_r.at[r, other], tp=partner)

    def forward_arrival(r, other):
        here = buf.at[other * 2 + 1 - core, part(r)]
        return remote(here, here, f_s.at[r, other], f_r.at[r, other], tp=partner)

    def piece(src, r):
        return kvs.at[src, r, :, side]

    def column_copy(r, k):
        return remote(piece(sp, r), piece(sp, r), z_s.at[r, k], i_r.at[sp, r], sp=sp + k * nx)

    def own_side(r, step):
        to = z * nx + lax.rem(x + step, nx)
        return remote(piece(sp, r), piece(sp, r), o_s.at[r, step], i_r.at[sp, r], sp=to)

    def relay(k, r, step):
        src = sp - k * nx
        to = z * nx + lax.rem(x + step, nx)
        return remote(piece(src, r), piece(src, r), x_s.at[k, r, step], i_r.at[src, r], sp=to)

    def arrival(src, r):
        return remote(piece(src, r), piece(src, r), z_s.at[r, 0], i_r.at[src, r], tp=partner)

    def share(src, r):
        return remote(piece(src, r), piece(src, r), d_s.at[src, r], d_r.at[src, r], tp=partner)

    def share_arrival(src, r):
        other = pl.ds(pl.multiple_of((1 - core) * (rank // 2), LANES), rank // 2)
        here = kvs.at[src, r, :, other]
        return remote(here, here, d_s.at[src, r], d_r.at[src, r], tp=partner)

    def halo_copy():
        return remote(tail, halo, h_s.at[0], h_r.at[0], sp=sp + 1)

    for r in range(count):
        tokens[r].wait()
        for step in range(1, ny):
            y_copy(r, step).start()
        own_copy(r).start()

    qt[...] = jnp.zeros_like(qt)
    loads[0].wait()
    vut[...] = vu[...].T
    loads[1].wait()
    for p in range(pairs):
        first, second = 2 * p * LANES, (2 * p + 1) * LANES
        upk[:, p * LANES : (p + 1) * LANES] = jnp.concatenate(
            [vkv[:, first : first + NOPE], vkv[:, second : second + NOPE]], axis=1
        )
    turned = vkv[...].T
    for h in range(heads):
        upvt[h * VDIM : (h + 1) * VDIM] = turned[h * LANES + NOPE : (h + 1) * LANES]

    def raise_keys(src, slot, span):
        count_here = len(span)
        lat = jnp.concatenate([kvs[src, r, : chunk] for r in span], axis=0)
        here = pl.ds(span[0] * chunk, count_here * chunk)
        kn[slot, here] = dot(lat, upk[...]).astype(BF)
        vt[slot, :, here] = dot_nt(upvt[...], lat).astype(BF)
        for r in span:
            packed = kvs[src, r, chunk:].astype(F32)
            tall = jnp.concatenate(
                [packed[:, g * LANES : (g + 1) * LANES] for g in range(ROPE // TURN)]
                + [jnp.zeros((LANES - ROPE, LANES), F32)],
                axis=0,
            )
            turn[slot, part(r)] = tall.T.astype(BF)

    def units(todo, slot, diagonal):
        peaks, ready = {}, {}
        size = len(todo)

        def keys(c):
            return (c + 1) * chunk if diagonal else rows

        def score(i):
            c, p = todo[i]
            k = keys(c)
            left = jnp.concatenate(
                [kn[slot, :k, p * LANES : (p + 1) * LANES], turn[slot, :k]], axis=1
            )
            s = dot(left, qt[c, p])
            if diagonal:
                last = s[k - chunk :]
                key = lax.broadcasted_iota(jnp.int32, last.shape, 0)
                query = lax.rem(lax.broadcasted_iota(jnp.int32, last.shape, 1), chunk)
                last = jnp.where(key <= query, last, NEGATIVE)
                s = last if k == chunk else jnp.concatenate([s[: k - chunk], last], axis=0)
            sbuf[i % (AHEAD + 2), :k] = s
            peaks[i] = jnp.max(s, axis=0, keepdims=True) * factor2

        def soften(i):
            c, p = todo[i]
            peak = peaks.pop(i)
            shrink = None
            if not diagonal:
                before = top[c, p]
                peak = jnp.maximum(before, peak)
                shrink = jnp.exp2(before - peak)
            w = jnp.exp2(sbuf[i % (AHEAD + 2), : keys(c)] * factor2 - peak)
            sums = jnp.sum(w, axis=0, keepdims=True)
            low[c, p] = sums if diagonal else low[c, p] * shrink + sums
            top[c, p] = peak
            ready[i] = (w.astype(BF), shrink)

        def gather(i):
            c, p = todo[i]
            w, shrink = ready.pop(i)
            o = dot(vt[slot, p * LANES : (p + 1) * LANES, : keys(c)], w)
            o = jnp.concatenate([o[:VDIM, :chunk], o[VDIM:, chunk:]], axis=1)
            acc[c, p] = o if diagonal else acc[c, p] * shrink + o

        for t in range(size + AHEAD + 1):
            if t < size:
                score(t)
            if 0 <= t - AHEAD < size:
                soften(t - AHEAD)
            if 0 <= t - AHEAD - 1 < size:
                gather(t - AHEAD - 1)

    def project(r):
        for step in range(1, ny):
            other = lax.rem(y + ny - step, ny)
            y_arrival(r, other).wait_recv()
            forward(r, other).start()
        own_arrival(r).wait_recv()
        for step in range(1, ny):
            forward_arrival(r, lax.rem(y + ny - step, ny)).wait_recv()
        if r == 0:
            for load in loads[2:5]:
                load.wait()
        here = part(r)
        wide = jnp.concatenate([buf[s, here] for s in range(n)], axis=1).astype(F32)
        factor = lax.rsqrt(jnp.sum(wide * wide, axis=1, keepdims=True) / (n * width) + EPSILON)
        scaled = (wide * pre[...]).astype(BF)
        flat = jnp.broadcast_to(factor, (chunk, LANES)).T[:1]
        cosine, sine = angle[: ROPE // 2, here], angle[ROPE // 2 :, here]

        def rotate(first, second):
            return jnp.concatenate(
                [first * cosine - second * sine, second * cosine + first * sine], axis=0
            )

        kv = dot(scaled, vk[...]) * factor
        kv = kv * lax.rsqrt(jnp.mean(kv * kv, axis=1, keepdims=True) + EPSILON) * kg[...]
        kvs[sp, r, :chunk] = kv.astype(BF)
        key = dot_nt(vr[...], scaled) * flat
        key = rotate(key[: ROPE // 2], key[ROPE // 2 :])
        kvs[sp, r, chunk:] = jnp.concatenate(
            [key[g * TURN : (g + 1) * TURN] for g in range(ROPE // TURN)], axis=1
        ).astype(BF)
        for k in range(1, nz):
            @pl.when(z + k < nz)
            def _(k=k):
                column_copy(r, k).start()
        for step in range(1, nx):
            @pl.when(x + step < nx)
            def _(step=step):
                own_side(r, step).start()

        if r == 0:
            loads[5].wait()
        q = dot(scaled, vq[...]) * factor
        gains = jnp.concatenate([qg[i : i + 1] for i in range(qg.shape[0])], axis=1)
        q = q * lax.rsqrt(jnp.mean(q * q, axis=1, keepdims=True) + EPSILON) * gains
        query = dot_nt(vut[...], q.astype(BF))
        for h in range(heads):
            p, low_half = h // 2, h % 2
            base = h * (NOPE + ROPE)
            span = slice(low_half * chunk, (low_half + 1) * chunk)
            qt[r, p, low_half * NOPE : (low_half + 1) * NOPE, span] = query[
                base : base + NOPE
            ].astype(BF)
            middle = base + NOPE + ROPE // 2
            qt[r, p, 2 * NOPE : 2 * NOPE + ROPE, span] = rotate(
                query[base + NOPE : middle], query[middle : base + NOPE + ROPE]
            ).astype(BF)

        if r == 0:
            for load in loads[6:9]:
                load.wait()
        inner = (dot(scaled, vi[...]) * factor).astype(BF).astype(F32)
        source = (dot(scaled, vs[...]) * factor).astype(BF).astype(F32)
        driven = (inner * source).astype(BF)
        ext[8 + r * chunk : 8 + (r + 1) * chunk] = driven.astype(F32)
        if r == count - 1:
            tail[...] = driven[chunk - HALO :]

            @pl.when(sp < nsp - 1)
            def _():
                halo_copy().start()
        outer[here] = (dot(scaled, vo[...]) * factor).astype(BF)
        raise_keys(sp, 0, [r])
        units([(r, p) for p in range(pairs)], 0, True)

    for r in range(count):
        project(r)

    items = z * nx + x

    def place_of(i):
        j = i - x
        level = jnp.where(j < 0, 0, j // nx + 1)
        turn_of = lax.rem(j + nx, nx)
        across_x = jnp.where(j < 0, i, lax.rem(x + turn_of, nx))
        column = jnp.logical_and(j >= 0, turn_of == 0)
        level = jnp.where(column, level, jnp.where(j < 0, 0, level))
        return (z - level) * nx + across_x, level, column

    def fetch(i):
        src, level, column = place_of(i)
        for r in range(count):
            arrival(src, r).wait_recv()
            share(src, r).start()

            @pl.when(column)
            def _(r=r):
                for step in range(1, nx):
                    relay(level, r, step).start()

    def take(i, slot):
        src, _, _ = place_of(i)
        for r in range(count):
            share_arrival(src, r).wait_recv()
        raise_keys(src, slot, list(range(count)))

    wave = jnp.minimum(items, WAVE)

    def whole(i, carry):
        fetch(i)
        take(i, 0)
        units([(c, p) for c in range(count) for p in range(pairs)], 0, False)
        return carry

    lax.fori_loop(0, items - wave, whole, 0)

    def ready(w, carry):
        fetch(items - wave + w)
        take(items - wave + w, w)
        return carry

    lax.fori_loop(0, wave, ready, 0)

    @pl.when(sp == 0)
    def _():
        ext[:8] = jnp.zeros((8, ext.shape[1]), F32)

    @pl.when(sp > 0)
    def _():
        remote(tail, halo, h_s.at[0], h_r.at[0], tp=partner).wait_recv()
        ext[:8] = halo[...].astype(F32)[HALO - 8 :]

    def product(r, dest):
        columns = pl.ds(pl.multiple_of(dest * width, width), width)
        return (
            dot(att[part(r), : heads * VDIM], va[:, columns])
            + dot(att[part(r), heads * VDIM :], vc[:, columns])
        ).astype(BF)

    def to_partner(r, step):
        return remote(
            away.at[step, part(r)], pin.at[step, part(r)], a_s.at[r, step], a_r.at[r, step], tp=partner
        )

    def across(r, step):
        to = lax.rem(y + step, ny) * 2 + core
        return remote(
            ysend.at[step, part(r)], yin.at[step, part(r)], b_s.at[r, step], b_r.at[r, step], tp=to
        )

    def home(r):
        return remote(peer.at[part(r)], pown.at[part(r)], p_s.at[r], p_r.at[r], tp=partner)

    def squares(r, step):
        return remote(
            sq.at[r], sqin.at[step, r], q_s.at[r, step], q_r.at[r, step], tp=lax.rem(tp + step, n)
        )

    for load in loads[9:]:
        load.wait()

    for c in range(count):
        def last(w, carry, c=c):
            units([(c, p) for p in range(pairs)], w, False)
            return carry

        lax.fori_loop(0, wave, last, 0)
        for p in range(pairs):
            value = acc[c, p] / low[c, p]
            both = jnp.concatenate([value[:, :chunk], value[:, chunk:]], axis=0)
            att[part(c), p * LANES : (p + 1) * LANES] = both.T.astype(BF)
            log = top[c, p] * math.log(2.0) + jnp.log(low[c, p])
            logs[2 * p : 2 * p + 1, part(c)] = log[:, :chunk]
            logs[2 * p + 1 : 2 * p + 2, part(c)] = log[:, chunk:]
        conv = jnp.zeros((chunk, ext.shape[1]), F32)
        for index in range(TAPS):
            start = 8 + c * chunk - (TAPS - 1) + index
            conv = conv + taps[index : index + 1].astype(F32) * ext[start : start + chunk]
        att[part(c), heads * VDIM :] = (outer[part(c)].astype(F32) * conv).astype(BF)
        for step in range(1, ny):
            dest = lax.rem(y + step, ny) * 2
            away[step, part(c)] = product(c, dest + 1 - core)
            to_partner(c, step).start()
            mine[step, part(c)] = product(c, dest + core)
        peer[part(c)] = product(c, partner)
        home(c).start()
        for step in range(1, ny):
            to_partner(c, step).wait_recv()
            ysend[step, part(c)] = (
                mine[step, part(c)].astype(F32) + pin[step, part(c)].astype(F32)
            ).astype(BF)
            across(c, step).start()
        total[part(c)] = product(c, tp).astype(F32)
    for r in range(count):
        home(r).wait_recv()
        value = total[part(r)] + pown[part(r)].astype(F32)
        for step in range(1, ny):
            across(r, step).wait_recv()
            value = value + yin[step, part(r)].astype(F32)
        total[part(r)] = value
        sums = jnp.sum(value * value, axis=1, keepdims=True)
        sq[r] = jnp.broadcast_to(sums, (chunk, LANES)).T[:8]
        for step in range(1, n):
            squares(r, step).start()
    for r in range(count):
        whole_sum = sq[r]
        for step in range(1, n):
            squares(r, step).wait_recv()
            whole_sum = whole_sum + sqin[step, r]
        scale = lax.rsqrt(whole_sum / (n * width) + EPSILON)
        column = jnp.broadcast_to(scale[:1], (LANES, chunk)).T[:, :1]
        out[part(r)] = (total[part(r)] * column * gain[...]).astype(BF)

    for r in range(count):
        own_copy(r).wait_send()
        home(r).wait_send()
        for step in range(1, ny):
            y_copy(r, step).wait_send()
            forward(r, lax.rem(y + step, ny)).wait_send()
            to_partner(r, step).wait_send()
            across(r, step).wait_send()
        for step in range(1, n):
            squares(r, step).wait_send()
        for k in range(1, nz):
            @pl.when(z + k < nz)
            def _(k=k, r=r):
                column_copy(r, k).wait_send()
        for step in range(1, nx):
            @pl.when(x + step < nx)
            def _(step=step, r=r):
                own_side(r, step).wait_send()

    @pl.when(sp < nsp - 1)
    def _():
        halo_copy().wait_send()

    def sent(i, carry):
        src, level, column = place_of(i)
        for r in range(count):
            share(src, r).wait_send()

            @pl.when(column)
            def _(r=r):
                for step in range(1, nx):
                    relay(level, r, step).wait_send()
        return carry

    lax.fori_loop(0, items, sent, 0)


DMA = pltpu.SemaphoreType.DMA


def angles(tokens):
    freqs = np.float32(THETA) ** (-np.arange(0, ROPE, 2, dtype=np.float32) / np.float32(ROPE))
    phase = freqs.astype(np.float32)[:, None] * np.arange(tokens, dtype=np.float32)[None, :]
    phase = phase.astype(np.float64)
    return np.concatenate([np.cos(phase), np.sin(phase)], axis=0).astype(np.float32)


def body(
    nsp, ntp,
    tokens, pre_gain, outer_gate_weight, inner_gate_weight, source_weight, conv_taps,
    q_down_weight, q_norm_gain, q_up_weight, kv_down_weight, rope_key_weight, kv_norm_gain,
    kv_up_weight, attn_out_weight, conv_out_weight, post_gain,
):
    rows, width = tokens.shape
    ny = ntp // 2
    nx = ny if nsp % ny == 0 else 1
    nz = nsp // nx
    chunk = LANES
    count = rows // chunk
    q_rank, rank = q_down_weight.shape[1], kv_down_weight.shape[1]
    channels = outer_gate_weight.shape[1]
    heads = q_up_weight.shape[1] // (NOPE + ROPE)
    pairs = heads // 2
    struct = jax.ShapeDtypeStruct
    v = pltpu.VMEM
    whole = pl.BlockSpec(memory_space=pltpu.VMEM)
    anywhere = pl.BlockSpec(memory_space=pl.ANY)
    rope_turned = rope_key_weight.T
    weights = (
        outer_gate_weight, inner_gate_weight, source_weight, q_down_weight, kv_down_weight,
        rope_turned, q_up_weight, kv_up_weight, attn_out_weight, conv_out_weight,
    )
    block = (ny, rows, width)
    return pl.pallas_call(
        functools.partial(layer_kernel, nz, nx, ntp, chunk, heads),
        out_shape=[struct((rows, width), BF), struct((heads, rows), F32)],
        in_specs=[anywhere] + [whole] * 5 + [anywhere] * (1 + len(weights)),
        out_specs=[whole] * 2,
        scratch_shapes=[v((ntp, rows, width), BF)]
        + [v(w.shape, BF) for w in weights]
        + [
            v((ROPE, rows), F32),
            v(q_up_weight.shape[::-1], BF),
            v((rank, heads * NOPE), BF), v((heads * VDIM, rank), BF),
            v((count, pairs, 2 * LANES, 2 * chunk), BF),
            v((nsp, count, chunk + TURN, rank), BF),
            v((WAVE, rows, heads * NOPE), BF), v((WAVE, rows, LANES), BF),
            v((WAVE, heads * VDIM, rows), BF),
            v((AHEAD + 2, rows, 2 * chunk), F32),
            v((count, pairs, VDIM, 2 * chunk), F32),
            v((count, pairs, 1, 2 * chunk), F32), v((count, pairs, 1, 2 * chunk), F32),
            v((rows, channels), BF), v((8 + rows, channels), F32),
            v((HALO, channels), BF), v((HALO, channels), BF),
            v((rows, heads * VDIM + channels), BF),
        ]
        + [v(block, BF)] * 5
        + [
            v((rows, width), BF), v((rows, width), BF), v((rows, width), F32),
            v((count, 8, chunk), F32), v((ntp, count, 8, chunk), F32),
            DMA((count,)), DMA((11,)), DMA((count,)), DMA((count,)),
            DMA((count, ny)), DMA((count, ny)), DMA((count, ny)), DMA((count, ny)),
            DMA((count, nz)), DMA((count, nx)), DMA((nz, count, nx)),
            DMA((nsp, count)), DMA((nsp, count)), DMA((nsp, count)), DMA((1,)), DMA((1,)),
            DMA((count, ny)), DMA((count, ny)), DMA((count, ny)), DMA((count, ny)),
            DMA((count,)), DMA((count,)), DMA((count, ntp)), DMA((count, ntp)),
        ],
        compiler_params=pltpu.CompilerParams(
            collective_id=0, has_side_effects=True, vmem_limit_bytes=60 * 1024 * 1024
        ),
        name="layer",
    )(
        tokens, pre_gain[None], q_norm_gain.reshape(-1, LANES), kv_norm_gain[None],
        post_gain[None], conv_taps, jnp.asarray(angles(nsp * rows)), *weights,
    )


def solution(mesh):
    placed = (
        P("sp", "tp"), P(), P(None, "tp"), P(None, "tp"), P(None, "tp"), P(None, "tp"), P(), P(),
        P(None, "tp"), P(), P(), P(), P(None, "tp"), P("tp", None), P("tp", None), P("tp"),
    )
    return jax.shard_map(
        functools.partial(body, mesh.shape["sp"], mesh.shape["tp"]),
        mesh=mesh,
        in_specs=placed,
        out_specs=(P("sp", "tp"), P("tp", "sp")),
        check_vma=False,
    )
```

```python
import functools
import math

import jax
import jax.numpy as jnp
import numpy as np
from jax import lax
from jax.experimental import pallas as pl
from jax.experimental.pallas import tpu as pltpu
from jax.sharding import PartitionSpec as P

NOPE = 64
ROPE = 32
VDIM = 64
TAPS = 3
LANES = 128
HALO = 16
TURN = 8
AHEAD = 2
WAVE = 1

EPSILON = 1e-06
THETA = 500000.0
NEGATIVE = -1e30
MESH = pl.DeviceIdType.MESH
BF = jnp.bfloat16
F32 = jnp.float32


def remote(src, dst, send, recv, **where):
    return pltpu.make_async_remote_copy(
        src_ref=src, dst_ref=dst, send_sem=send, recv_sem=recv, device_id=where, device_id_type=MESH
    )


def dot(a, b):
    return jnp.dot(a, b, preferred_element_type=F32)


def dot_nt(a, b):
    return lax.dot_general(a, b, (((1,), (1,)), ((), ())), preferred_element_type=F32)


def layer_kernel(
    nz, nx, n, chunk, heads,
    tok, pre, qg, kg, gain, taps, table, wo, wi, ws, wq, wk, wr, wu, wkv, wa, wc,
    out, logs,
    buf, vo, vi, vs, vq, vk, vr, vu, vkv, va, vc, angle,
    vut, upk, upvt, qt, kvs, kn, turn, vt, sbuf, acc, top, low,
    outer, ext, tail, halo, att,
    away, mine, pin, ysend, yin, peer, pown, total, sq, sqin,
    t_s, w_s, own_s, own_r, y_s, y_r, f_s, f_r,
    z_s, o_s, x_s, i_r, d_s, d_r, h_s, h_r,
    a_s, a_r, b_s, b_r, p_s, p_r, q_s, q_r,
):
    sp, tp = lax.axis_index("sp"), lax.axis_index("tp")
    nsp = nz * nx
    z, x = sp // nx, lax.rem(sp, nx)
    ny = n // 2
    y, core = tp // 2, lax.rem(tp, 2)
    partner = tp + 1 - 2 * core
    rows, width = tok.shape
    count = rows // chunk
    pairs = heads // 2
    rank = wkv.shape[0]
    factor2 = (NOPE + ROPE) ** (-0.5) * math.log2(math.e)
    side = pl.ds(pl.multiple_of(core * (rank // 2), LANES), rank // 2)

    def part(r):
        return pl.ds(r * chunk, chunk)

    tokens = [
        pltpu.make_async_copy(tok.at[part(r)], buf.at[tp, part(r)], t_s.at[r]) for r in range(count)
    ]
    place = pl.ds(pl.multiple_of(sp * rows, LANES), rows)
    pairs_of = (
        (wu, vu), (wkv, vkv), (table.at[:, place], angle), (wk, vk), (wr, vr), (wq, vq),
        (wi, vi), (ws, vs), (wo, vo), (wa, va), (wc, vc),
    )
    loads = [pltpu.make_async_copy(a, b, w_s.at[i]) for i, (a, b) in enumerate(pairs_of)]
    for token in tokens:
        token.start()

    barrier = pltpu.get_barrier_semaphore()

    def greet(**where):
        pl.semaphore_signal(barrier, inc=1, device_id=where, device_id_type=MESH)

    for step in range(1, n):
        greet(tp=lax.rem(tp + step, n))
    for step in range(1, nz):
        greet(sp=lax.rem(z + step, nz) * nx + x)
    for step in range(1, nx):
        greet(sp=z * nx + lax.rem(x + step, nx))
    greet(sp=lax.rem(sp + 1, nsp))
    greet(sp=lax.rem(sp + nsp - 1, nsp))
    for load in loads:
        load.start()
    with jax.named_scope("barrier"):
        pl.semaphore_wait(barrier, n - 1 + nz - 1 + nx - 1 + 2)

    def y_copy(r, step):
        to = lax.rem(y + step, ny) * 2 + core
        here = buf.at[tp, part(r)]
        return remote(here, here, y_s.at[r, step], y_r.at[r, y], tp=to)

    def y_arrival(r, other):
        here = buf.at[other * 2 + core, part(r)]
        return remote(here, here, y_s.at[r, 0], y_r.at[r, other], tp=partner)

    def own_copy(r):
        here = buf.at[tp, part(r)]
        return remote(here, here, own_s.at[r], own_r.at[r], tp=partner)

    def own_arrival(r):
        here = buf.at[partner, part(r)]
        return remote(here, here, own_s.at[r], own_r.at[r], tp=partner)

    def forward(r, other):
        here = buf.at[other * 2 + core, part(r)]
        return remote(here, here, f_s.at[r, other], f_r.at[r, other], tp=partner)

    def forward_arrival(r, other):
        here = buf.at[other * 2 + 1 - core, part(r)]
        return remote(here, here, f_s.at[r, other], f_r.at[r, other], tp=partner)

    def piece(src, r):
        return kvs.at[src, r, :, side]

    def column_copy(r, k):
        return remote(piece(sp, r), piece(sp, r), z_s.at[r, k], i_r.at[sp, r], sp=sp + k * nx)

    def own_side(r, step):
        to = z * nx + lax.rem(x + step, nx)
        return remote(piece(sp, r), piece(sp, r), o_s.at[r, step], i_r.at[sp, r], sp=to)

    def relay(k, r, step):
        src = sp - k * nx
        to = z * nx + lax.rem(x + step, nx)
        return remote(piece(src, r), piece(src, r), x_s.at[k, r, step], i_r.at[src, r], sp=to)

    def arrival(src, r):
        return remote(piece(src, r), piece(src, r), z_s.at[r, 0], i_r.at[src, r], tp=partner)

    def share(src, r):
        return remote(piece(src, r), piece(src, r), d_s.at[src, r], d_r.at[src, r], tp=partner)

    def share_arrival(src, r):
        other = pl.ds(pl.multiple_of((1 - core) * (rank // 2), LANES), rank // 2)
        here = kvs.at[src, r, :, other]
        return remote(here, here, d_s.at[src, r], d_r.at[src, r], tp=partner)

    def halo_copy():
        return remote(tail, halo, h_s.at[0], h_r.at[0], sp=sp + 1)

    with jax.named_scope("sendtok"):
        for r in range(count):
            tokens[r].wait()
            for step in range(1, ny):
                y_copy(r, step).start()
            own_copy(r).start()

    with jax.named_scope("wturn"):
        qt[...] = jnp.zeros_like(qt)
        loads[0].wait()
        vut[...] = vu[...].T
    with jax.named_scope("wload1"):
        loads[1].wait()
    for p in range(pairs):
        first, second = 2 * p * LANES, (2 * p + 1) * LANES
        upk[:, p * LANES : (p + 1) * LANES] = jnp.concatenate(
            [vkv[:, first : first + NOPE], vkv[:, second : second + NOPE]], axis=1
        )
    turned = vkv[...].T
    for h in range(heads):
        upvt[h * VDIM : (h + 1) * VDIM] = turned[h * LANES + NOPE : (h + 1) * LANES]

    def raise_keys(src, slot, span):
        count_here = len(span)
        lat = jnp.concatenate([kvs[src, r, : chunk] for r in span], axis=0)
        here = pl.ds(span[0] * chunk, count_here * chunk)
        kn[slot, here] = dot(lat, upk[...]).astype(BF)
        vt[slot, :, here] = dot_nt(upvt[...], lat).astype(BF)
        for r in span:
            packed = kvs[src, r, chunk:].astype(F32)
            tall = jnp.concatenate(
                [packed[:, g * LANES : (g + 1) * LANES] for g in range(ROPE // TURN)]
                + [jnp.zeros((LANES - ROPE, LANES), F32)],
                axis=0,
            )
            turn[slot, part(r)] = tall.T.astype(BF)

    def units(todo, slot, diagonal):
        peaks, ready = {}, {}
        size = len(todo)

        def keys(c):
            return (c + 1) * chunk if diagonal else rows

        def score(i):
            c, p = todo[i]
            k = keys(c)
            left = jnp.concatenate(
                [kn[slot, :k, p * LANES : (p + 1) * LANES], turn[slot, :k]], axis=1
            )
            s = dot(left, qt[c, p])
            if diagonal:
                last = s[k - chunk :]
                key = lax.broadcasted_iota(jnp.int32, last.shape, 0)
                query = lax.rem(lax.broadcasted_iota(jnp.int32, last.shape, 1), chunk)
                last = jnp.where(key <= query, last, NEGATIVE)
                s = last if k == chunk else jnp.concatenate([s[: k - chunk], last], axis=0)
            sbuf[i % (AHEAD + 2), :k] = s
            peaks[i] = jnp.max(s, axis=0, keepdims=True) * factor2

        def soften(i):
            c, p = todo[i]
            peak = peaks.pop(i)
            shrink = None
            if not diagonal:
                before = top[c, p]
                peak = jnp.maximum(before, peak)
                shrink = jnp.exp2(before - peak)
            w = jnp.exp2(sbuf[i % (AHEAD + 2), : keys(c)] * factor2 - peak)
            sums = jnp.sum(w, axis=0, keepdims=True)
            low[c, p] = sums if diagonal else low[c, p] * shrink + sums
            top[c, p] = peak
            ready[i] = (w.astype(BF), shrink)

        def gather(i):
            c, p = todo[i]
            w, shrink = ready.pop(i)
            o = dot(vt[slot, p * LANES : (p + 1) * LANES, : keys(c)], w)
            o = jnp.concatenate([o[:VDIM, :chunk], o[VDIM:, chunk:]], axis=1)
            acc[c, p] = o if diagonal else acc[c, p] * shrink + o

        for t in range(size + AHEAD + 1):
            if t < size:
                score(t)
            if 0 <= t - AHEAD < size:
                soften(t - AHEAD)
            if 0 <= t - AHEAD - 1 < size:
                gather(t - AHEAD - 1)

    items = z * nx + x

    def place_of(i):
        j = i - x
        turn_of = lax.rem(j + nx, nx)
        across_x = jnp.where(j < 0, i, lax.rem(x + turn_of, nx))
        level = jnp.where(j < 0, 0, j // nx + 1)
        column = jnp.logical_and(j >= 0, turn_of == 0)
        return (z - level) * nx + across_x, column

    def pump(k, r):
        @pl.when(k <= z)
        def _():
            src = sp - k * nx
            arrival(src, r).wait_recv()
            share(src, r).start()
            for step in range(1, nx):
                relay(k, r, step).start()

    def fetch(i):
        src, column = place_of(i)

        @pl.when(jnp.logical_and(i < items, jnp.logical_not(column)))
        def _():
            for r in range(count):
                arrival(src, r).wait_recv()
                share(src, r).start()

    def take(i, slot):
        src, _ = place_of(i)
        with jax.named_scope("sharewait"):
            for r in range(count):
                share_arrival(src, r).wait_recv()
        raise_keys(src, slot, list(range(count)))
        with jax.named_scope("pump"):
            @pl.when(i > 0)
            def _():
                for r in range(count - 1):
                    pump(i + 2, r)

            pump(i + 2, count - 1)
        with jax.named_scope("fetch"):
            fetch(i + 1)

    def pass_on(r):
        for step in range(1, ny):
            other = lax.rem(y + ny - step, ny)
            y_arrival(r, other).wait_recv()
            forward(r, other).start()

    def project(r):
        with jax.named_scope(f"tokwait{r}"):
            if r == 0:
                pass_on(r)
            own_arrival(r).wait_recv()
            for step in range(1, ny):
                forward_arrival(r, lax.rem(y + ny - step, ny)).wait_recv()
        if r == 0:
            with jax.named_scope("wload2"):
                for load in loads[2:5]:
                    load.wait()
        here = part(r)
        wide = jnp.concatenate([buf[s, here] for s in range(n)], axis=1).astype(F32)
        factor = lax.rsqrt(jnp.sum(wide * wide, axis=1, keepdims=True) / (n * width) + EPSILON)
        scaled = (wide * pre[...]).astype(BF)
        flat = jnp.broadcast_to(factor, (chunk, LANES)).T[:1]
        cosine, sine = angle[: ROPE // 2, here], angle[ROPE // 2 :, here]

        def rotate(first, second):
            return jnp.concatenate(
                [first * cosine - second * sine, second * cosine + first * sine], axis=0
            )

        kv = dot(scaled, vk[...]) * factor
        kv = kv * lax.rsqrt(jnp.mean(kv * kv, axis=1, keepdims=True) + EPSILON) * kg[...]
        kvs[sp, r, :chunk] = kv.astype(BF)
        key = dot_nt(vr[...], scaled) * flat
        key = rotate(key[: ROPE // 2], key[ROPE // 2 :])
        kvs[sp, r, chunk:] = jnp.concatenate(
            [key[g * TURN : (g + 1) * TURN] for g in range(ROPE // TURN)], axis=1
        ).astype(BF)
        for k in range(1, nz):
            @pl.when(z + k < nz)
            def _(k=k):
                column_copy(r, k).start()
        for step in range(1, nx):
            @pl.when(x + step < nx)
            def _(step=step):
                own_side(r, step).start()

        if r == 0:
            with jax.named_scope("wload5"):
                loads[5].wait()
        q = dot(scaled, vq[...]) * factor
        gains = jnp.concatenate([qg[i : i + 1] for i in range(qg.shape[0])], axis=1)
        q = q * lax.rsqrt(jnp.mean(q * q, axis=1, keepdims=True) + EPSILON) * gains
        with jax.named_scope("passon"):
            if r + 1 < count:
                pass_on(r + 1)
            else:
                for k in range(1, min(nz, 3)):
                    for early in range(count - 2):
                        pump(k, early)
        query = dot_nt(vut[...], q.astype(BF))
        for h in range(heads):
            p, low_half = h // 2, h % 2
            base = h * (NOPE + ROPE)
            span = slice(low_half * chunk, (low_half + 1) * chunk)
            qt[r, p, low_half * NOPE : (low_half + 1) * NOPE, span] = query[
                base : base + NOPE
            ].astype(BF)
            middle = base + NOPE + ROPE // 2
            qt[r, p, 2 * NOPE : 2 * NOPE + ROPE, span] = rotate(
                query[base + NOPE : middle], query[middle : base + NOPE + ROPE]
            ).astype(BF)

        if r == 0:
            with jax.named_scope("wload6"):
                for load in loads[6:9]:
                    load.wait()
        inner = (dot(scaled, vi[...]) * factor).astype(BF).astype(F32)
        source = (dot(scaled, vs[...]) * factor).astype(BF).astype(F32)
        driven = (inner * source).astype(BF)
        ext[8 + r * chunk : 8 + (r + 1) * chunk] = driven.astype(F32)
        if r == count - 1:
            tail[...] = driven[chunk - HALO :]

            @pl.when(sp < nsp - 1)
            def _():
                halo_copy().start()
        outer[here] = (dot(scaled, vo[...]) * factor).astype(BF)
        if r == count - 1:
            with jax.named_scope("prefetch"):
                for k in range(1, min(nz, 3)):
                    pump(k, count - 2)
                fetch(0)
                pump(1, count - 1)
        with jax.named_scope(f"diag{r}"):
            raise_keys(sp, 0, [r])
            units([(r, p) for p in range(pairs)], 0, True)

    for r in range(count):
        project(r)

    wave = jnp.minimum(items, WAVE)

    def whole(i, carry):
        take(i, 0)
        with jax.named_scope("units"):
          units([(c, p) for c in range(count) for p in range(pairs)], 0, False)
        return carry

    lax.fori_loop(0, items - wave, whole, 0)

    def ready(w, carry):
        take(items - wave + w, w)
        return carry

    lax.fori_loop(0, wave, ready, 0)

    @pl.when(sp == 0)
    def _():
        ext[:8] = jnp.zeros((8, ext.shape[1]), F32)

    @pl.when(sp > 0)
    def _():
        remote(tail, halo, h_s.at[0], h_r.at[0], tp=partner).wait_recv()
        ext[:8] = halo[...].astype(F32)[HALO - 8 :]

    def product(r, dest):
        columns = pl.ds(pl.multiple_of(dest * width, width), width)
        return (
            dot(att[part(r), : heads * VDIM], va[:, columns])
            + dot(att[part(r), heads * VDIM :], vc[:, columns])
        ).astype(BF)

    def to_partner(r, step):
        return remote(
            away.at[step, part(r)], pin.at[step, part(r)], a_s.at[r, step], a_r.at[r, step], tp=partner
        )

    def across(r, step):
        to = lax.rem(y + step, ny) * 2 + core
        return remote(
            ysend.at[step, part(r)], yin.at[step, part(r)], b_s.at[r, step], b_r.at[r, step], tp=to
        )

    def home(r):
        return remote(peer.at[part(r)], pown.at[part(r)], p_s.at[r], p_r.at[r], tp=partner)

    def squares(r, step):
        return remote(
            sq.at[r], sqin.at[step, r], q_s.at[r, step], q_r.at[r, step], tp=lax.rem(tp + step, n)
        )

    for load in loads[9:]:
        load.wait()

    def send_on(c):
        for step in range(1, ny):
            with jax.named_scope("partnerwait"):
                to_partner(c, step).wait_recv()
            ysend[step, part(c)] = (
                mine[step, part(c)].astype(F32) + pin[step, part(c)].astype(F32)
            ).astype(BF)
            across(c, step).start()

    for c in range(count):
        def last(w, carry, c=c):
            with jax.named_scope("lastunits"):
                units([(c, p) for p in range(pairs)], w, False)
            return carry

        lax.fori_loop(0, wave, last, 0)
        if c > 0:
            send_on(c - 1)
        for p in range(pairs):
            value = acc[c, p] / low[c, p]
            both = jnp.concatenate([value[:, :chunk], value[:, chunk:]], axis=0)
            att[part(c), p * LANES : (p + 1) * LANES] = both.T.astype(BF)
            log = top[c, p] * math.log(2.0) + jnp.log(low[c, p])
            logs[2 * p : 2 * p + 1, part(c)] = log[:, :chunk]
            logs[2 * p + 1 : 2 * p + 2, part(c)] = log[:, chunk:]
        conv = jnp.zeros((chunk, ext.shape[1]), F32)
        for index in range(TAPS):
            start = 8 + c * chunk - (TAPS - 1) + index
            conv = conv + taps[index : index + 1].astype(F32) * ext[start : start + chunk]
        att[part(c), heads * VDIM :] = (outer[part(c)].astype(F32) * conv).astype(BF)
        for step in range(1, ny):
            dest = lax.rem(y + step, ny) * 2
            away[step, part(c)] = product(c, dest + 1 - core)
            to_partner(c, step).start()
            mine[step, part(c)] = product(c, dest + core)
        peer[part(c)] = product(c, partner)
        home(c).start()
        total[part(c)] = product(c, tp).astype(F32)
        if c == count - 1:
            send_on(c)
    for r in range(count):
        with jax.named_scope("homewait"):
            home(r).wait_recv()
        value = total[part(r)] + pown[part(r)].astype(F32)
        for step in range(1, ny):
            with jax.named_scope("acrosswait"):
                across(r, step).wait_recv()
            value = value + yin[step, part(r)].astype(F32)
        total[part(r)] = value
        sums = jnp.sum(value * value, axis=1, keepdims=True)
        sq[r] = jnp.broadcast_to(sums, (chunk, LANES)).T[:8]
        for step in range(1, n):
            squares(r, step).start()
    for r in range(count):
        whole_sum = sq[r]
        for step in range(1, n):
            with jax.named_scope("sqwait"):
                squares(r, step).wait_recv()
            whole_sum = whole_sum + sqin[step, r]
        scale = lax.rsqrt(whole_sum / (n * width) + EPSILON)
        column = jnp.broadcast_to(scale[:1], (LANES, chunk)).T[:, :1]
        out[part(r)] = (total[part(r)] * column * gain[...]).astype(BF)

    with jax.named_scope("endsends"):
        own_copy(0).wait_send()
    for r in range(count):
        if r > 0:
            own_copy(r).wait_send()
        home(r).wait_send()
        for step in range(1, ny):
            y_copy(r, step).wait_send()
            forward(r, lax.rem(y + step, ny)).wait_send()
            to_partner(r, step).wait_send()
            across(r, step).wait_send()
        for step in range(1, n):
            squares(r, step).wait_send()
        for k in range(1, nz):
            @pl.when(z + k < nz)
            def _(k=k, r=r):
                column_copy(r, k).wait_send()
        for step in range(1, nx):
            @pl.when(x + step < nx)
            def _(step=step, r=r):
                own_side(r, step).wait_send()

    @pl.when(sp < nsp - 1)
    def _():
        halo_copy().wait_send()

    def sent(i, carry):
        src, _ = place_of(i)
        for r in range(count):
            share(src, r).wait_send()
        return carry

    lax.fori_loop(0, items, sent, 0)

    def relayed(k, carry):
        for r in range(count):
            for step in range(1, nx):
                relay(k, r, step).wait_send()
        return carry

    lax.fori_loop(1, z + 1, relayed, 0)


DMA = pltpu.SemaphoreType.DMA


def angles(tokens):
    freqs = np.float32(THETA) ** (-np.arange(0, ROPE, 2, dtype=np.float32) / np.float32(ROPE))
    phase = freqs.astype(np.float32)[:, None] * np.arange(tokens, dtype=np.float32)[None, :]
    phase = phase.astype(np.float64)
    return np.concatenate([np.cos(phase), np.sin(phase)], axis=0).astype(np.float32)


def body(
    nsp, ntp,
    tokens, pre_gain, outer_gate_weight, inner_gate_weight, source_weight, conv_taps,
    q_down_weight, q_norm_gain, q_up_weight, kv_down_weight, rope_key_weight, kv_norm_gain,
    kv_up_weight, attn_out_weight, conv_out_weight, post_gain,
):
    rows, width = tokens.shape
    ny = ntp // 2
    nx = ny if nsp % ny == 0 else 1
    nz = nsp // nx
    chunk = LANES
    count = rows // chunk
    q_rank, rank = q_down_weight.shape[1], kv_down_weight.shape[1]
    channels = outer_gate_weight.shape[1]
    heads = q_up_weight.shape[1] // (NOPE + ROPE)
    pairs = heads // 2
    struct = jax.ShapeDtypeStruct
    v = pltpu.VMEM
    whole = pl.BlockSpec(memory_space=pltpu.VMEM)
    anywhere = pl.BlockSpec(memory_space=pl.ANY)
    rope_turned = rope_key_weight.T
    weights = (
        outer_gate_weight, inner_gate_weight, source_weight, q_down_weight, kv_down_weight,
        rope_turned, q_up_weight, kv_up_weight, attn_out_weight, conv_out_weight,
    )
    block = (ny, rows, width)
    return pl.pallas_call(
        functools.partial(layer_kernel, nz, nx, ntp, chunk, heads),
        out_shape=[v((rows, width), BF), v((heads, rows), F32)],
        in_specs=[anywhere] + [whole] * 5 + [anywhere] * (1 + len(weights)),
        out_specs=[whole] * 2,
        scratch_shapes=[v((ntp, rows, width), BF)]
        + [v(w.shape, BF) for w in weights]
        + [
            v((ROPE, rows), F32),
            v(q_up_weight.shape[::-1], BF),
            v((rank, heads * NOPE), BF), v((heads * VDIM, rank), BF),
            v((count, pairs, 2 * LANES, 2 * chunk), BF),
            v((nsp, count, chunk + TURN, rank), BF),
            v((WAVE, rows, heads * NOPE), BF), v((WAVE, rows, LANES), BF),
            v((WAVE, heads * VDIM, rows), BF),
            v((AHEAD + 2, rows, 2 * chunk), F32),
            v((count, pairs, VDIM, 2 * chunk), F32),
            v((count, pairs, 1, 2 * chunk), F32), v((count, pairs, 1, 2 * chunk), F32),
            v((rows, channels), BF), v((8 + rows, channels), F32),
            v((HALO, channels), BF), v((HALO, channels), BF),
            v((rows, heads * VDIM + channels), BF),
        ]
        + [v(block, BF)] * 5
        + [
            v((rows, width), BF), v((rows, width), BF), v((rows, width), F32),
            v((count, 8, chunk), F32), v((ntp, count, 8, chunk), F32),
            DMA((count,)), DMA((11,)), DMA((count,)), DMA((count,)),
            DMA((count, ny)), DMA((count, ny)), DMA((count, ny)), DMA((count, ny)),
            DMA((count, nz)), DMA((count, nx)), DMA((nz, count, nx)),
            DMA((nsp, count)), DMA((nsp, count)), DMA((nsp, count)), DMA((1,)), DMA((1,)),
            DMA((count, ny)), DMA((count, ny)), DMA((count, ny)), DMA((count, ny)),
            DMA((count,)), DMA((count,)), DMA((count, ntp)), DMA((count, ntp)),
        ],
        compiler_params=pltpu.CompilerParams(
            collective_id=0, has_side_effects=True, vmem_limit_bytes=60 * 1024 * 1024
        ),
        name="layer",
    )(
        tokens, pre_gain[None], q_norm_gain.reshape(-1, LANES), kv_norm_gain[None],
        post_gain[None], conv_taps, jnp.asarray(angles(nsp * rows)), *weights,
    )


def solution(mesh):
    placed = (
        P("sp", "tp"), P(), P(None, "tp"), P(None, "tp"), P(None, "tp"), P(None, "tp"), P(), P(),
        P(None, "tp"), P(), P(), P(), P(None, "tp"), P("tp", None), P("tp", None), P("tp"),
    )
    return jax.shard_map(
        functools.partial(body, mesh.shape["sp"], mesh.shape["tp"]),
        mesh=mesh,
        in_specs=placed,
        out_specs=(P("sp", "tp"), P("tp", "sp")),
        check_vma=False,
    )
```

```python
import functools
import math

import jax
import jax.numpy as jnp
import numpy as np
from jax import lax
from jax.experimental import pallas as pl
from jax.experimental.pallas import tpu as pltpu
from jax.sharding import PartitionSpec as P

NOPE = 64
ROPE = 32
VDIM = 64
TAPS = 3
LANES = 128
HALO = 16
TURN = 8
AHEAD = 2
WAVE = 3

EPSILON = 1e-06
THETA = 500000.0
NEGATIVE = -1e30
MESH = pl.DeviceIdType.MESH
BF = jnp.bfloat16
F32 = jnp.float32


def remote(src, dst, send, recv, **where):
    return pltpu.make_async_remote_copy(
        src_ref=src, dst_ref=dst, send_sem=send, recv_sem=recv, device_id=where, device_id_type=MESH
    )


def dot(a, b):
    return jnp.dot(a, b, preferred_element_type=F32)


def dot_nt(a, b):
    return lax.dot_general(a, b, (((1,), (1,)), ((), ())), preferred_element_type=F32)


def layer_kernel(
    nz, nx, n, chunk, heads,
    tok, pre, qg, kg, gain, taps, table, wo, wi, ws, wq, wk, wr, wu, wkv, wa, wc,
    out, logs,
    buf, vo, vi, vs, vq, vk, vr, vu, vkv, va, vc, angle,
    vut, upk, upvt, qt, kvs, kn, turn, vt, sbuf, acc, top, low,
    scale_of, factors, outer, ext, tail, halo, att,
    away, mine, pin, ysend, yin, peer, pown, total, sq, sqin,
    t_s, w_s, own_s, own_r, y_s, y_r, f_s, f_r,
    z_s, o_s, x_s, i_r, d_s, d_r, h_s, h_r,
    a_s, a_r, b_s, b_r, p_s, p_r, q_s, q_r,
):
    sp, tp = lax.axis_index("sp"), lax.axis_index("tp")
    nsp = nz * nx
    z, x = sp // nx, lax.rem(sp, nx)
    ny = n // 2
    y, core = tp // 2, lax.rem(tp, 2)
    partner = tp + 1 - 2 * core
    rows, width = tok.shape
    count = rows // chunk
    pairs = heads // 2
    rank = wkv.shape[0]
    factor2 = (NOPE + ROPE) ** (-0.5) * math.log2(math.e)
    side = pl.ds(pl.multiple_of(core * (rank // 2), LANES), rank // 2)

    def part(r):
        return pl.ds(r * chunk, chunk)

    tokens = [
        pltpu.make_async_copy(tok.at[part(r)], buf.at[tp, part(r)], t_s.at[r]) for r in range(count)
    ]
    place = pl.ds(pl.multiple_of(sp * rows, LANES), rows)
    pairs_of = (
        (wu, vu), (wkv, vkv), (table.at[:, place], angle), (wk, vk), (wr, vr), (wq, vq),
        (wi, vi), (ws, vs), (wo, vo), (wa, va), (wc, vc),
    )
    loads = [pltpu.make_async_copy(a, b, w_s.at[i]) for i, (a, b) in enumerate(pairs_of)]
    for token in tokens:
        token.start()

    barrier = pltpu.get_barrier_semaphore()

    def greet(**where):
        pl.semaphore_signal(barrier, inc=1, device_id=where, device_id_type=MESH)

    for step in range(1, n):
        greet(tp=lax.rem(tp + step, n))
    greet(sp=lax.rem(z + 1, nz) * nx + x)
    greet(sp=lax.rem(z + nz - 1, nz) * nx + x)
    for step in range(1, nx):
        greet(sp=z * nx + lax.rem(x + step, nx))
    greet(sp=lax.rem(sp + 1, nsp))
    greet(sp=lax.rem(sp + nsp - 1, nsp))
    for load in loads:
        load.start()
    with jax.named_scope("barrier"):
        pl.semaphore_wait(barrier, n - 1 + 2 + nx - 1 + 2)

    def y_copy(r, step):
        to = lax.rem(y + step, ny) * 2 + core
        here = buf.at[tp, part(r)]
        return remote(here, here, y_s.at[r, step], y_r.at[r, y], tp=to)

    def y_arrival(r, other):
        here = buf.at[other * 2 + core, part(r)]
        return remote(here, here, y_s.at[r, 0], y_r.at[r, other], tp=partner)

    def own_copy(r):
        here = buf.at[tp, part(r)]
        return remote(here, here, own_s.at[r], own_r.at[r], tp=partner)

    def own_arrival(r):
        here = buf.at[partner, part(r)]
        return remote(here, here, own_s.at[r], own_r.at[r], tp=partner)

    def forward(r, other):
        here = buf.at[other * 2 + core, part(r)]
        return remote(here, here, f_s.at[r, other], f_r.at[r, other], tp=partner)

    def forward_arrival(r, other):
        here = buf.at[other * 2 + 1 - core, part(r)]
        return remote(here, here, f_s.at[r, other], f_r.at[r, other], tp=partner)

    def piece(src, r):
        return kvs.at[src, r, :, side]

    def up_copy(k, r):
        src = sp - k * nx
        return remote(piece(src, r), piece(src, r), z_s.at[k, r], i_r.at[src, r], sp=sp + nx)

    def own_side(r, step):
        to = z * nx + lax.rem(x + step, nx)
        return remote(piece(sp, r), piece(sp, r), o_s.at[r, step], i_r.at[sp, r], sp=to)

    def relay(k, r, step):
        src = sp - k * nx
        to = z * nx + lax.rem(x + step, nx)
        return remote(piece(src, r), piece(src, r), x_s.at[k, r, step], i_r.at[src, r], sp=to)

    def arrival(src, r):
        return remote(piece(src, r), piece(src, r), z_s.at[0, r], i_r.at[src, r], tp=partner)

    def share(src, r):
        return remote(piece(src, r), piece(src, r), d_s.at[src, r], d_r.at[src, r], tp=partner)

    def share_arrival(src, r):
        other = pl.ds(pl.multiple_of((1 - core) * (rank // 2), LANES), rank // 2)
        here = kvs.at[src, r, :, other]
        return remote(here, here, d_s.at[src, r], d_r.at[src, r], tp=partner)

    def halo_copy():
        return remote(tail, halo, h_s.at[0], h_r.at[0], sp=sp + 1)

    with jax.named_scope("sendtok"):
        for r in range(count):
            tokens[r].wait()
            for step in range(1, ny):
                y_copy(r, step).start()
            own_copy(r).start()

    with jax.named_scope("wturn"):
        qt[...] = jnp.zeros_like(qt)
        loads[0].wait()
        vut[...] = vu[...].T
    with jax.named_scope("wload1"):
        loads[1].wait()
    for p in range(pairs):
        first, second = 2 * p * LANES, (2 * p + 1) * LANES
        upk[:, p * LANES : (p + 1) * LANES] = jnp.concatenate(
            [vkv[:, first : first + NOPE], vkv[:, second : second + NOPE]], axis=1
        )
    turned = vkv[...].T
    for h in range(heads):
        upvt[h * VDIM : (h + 1) * VDIM] = turned[h * LANES + NOPE : (h + 1) * LANES]

    def raise_keys(src, slot, span):
        count_here = len(span)
        lat = jnp.concatenate([kvs[src, r, : chunk] for r in span], axis=0)
        here = pl.ds(span[0] * chunk, count_here * chunk)
        kn[slot, here] = dot(lat, upk[...]).astype(BF)
        vt[slot, :, here] = dot_nt(upvt[...], lat).astype(BF)
        for r in span:
            packed = kvs[src, r, chunk:].astype(F32)
            tall = jnp.concatenate(
                [packed[:, g * LANES : (g + 1) * LANES] for g in range(ROPE // TURN)]
                + [jnp.zeros((LANES - ROPE, LANES), F32)],
                axis=0,
            )
            turn[slot, part(r)] = tall.T.astype(BF)

    def units(todo, diagonal):
        peaks, ready = {}, {}
        size = len(todo)

        def keys(c):
            return (c + 1) * chunk if diagonal else rows

        def score(i):
            c, p, slot = todo[i]
            k = keys(c)
            left = jnp.concatenate(
                [kn[slot, :k, p * LANES : (p + 1) * LANES], turn[slot, :k]], axis=1
            )
            s = dot(left, qt[c, p])
            if diagonal:
                last = s[k - chunk :]
                key = lax.broadcasted_iota(jnp.int32, last.shape, 0)
                query = lax.rem(lax.broadcasted_iota(jnp.int32, last.shape, 1), chunk)
                last = jnp.where(key <= query, last, NEGATIVE)
                s = last if k == chunk else jnp.concatenate([s[: k - chunk], last], axis=0)
            sbuf[i % (AHEAD + 2), :k] = s
            peaks[i] = jnp.max(s, axis=0, keepdims=True) * factor2

        def soften(i):
            c, p, slot = todo[i]
            peak = peaks.pop(i)
            shrink = None
            if not diagonal:
                before = top[c, p]
                peak = jnp.maximum(before, peak)
                shrink = jnp.exp2(before - peak)
            w = jnp.exp2(sbuf[i % (AHEAD + 2), : keys(c)] * factor2 - peak)
            sums = jnp.sum(w, axis=0, keepdims=True)
            low[c, p] = sums if diagonal else low[c, p] * shrink + sums
            top[c, p] = peak
            ready[i] = (w.astype(BF), shrink)

        def gather(i):
            c, p, slot = todo[i]
            w, shrink = ready.pop(i)
            o = dot(vt[slot, p * LANES : (p + 1) * LANES, : keys(c)], w)
            o = jnp.concatenate([o[:VDIM, :chunk], o[VDIM:, chunk:]], axis=1)
            acc[c, p] = o if diagonal else acc[c, p] * shrink + o

        for t in range(size + AHEAD + 1):
            if t < size:
                score(t)
            if 0 <= t - AHEAD < size:
                soften(t - AHEAD)
            if 0 <= t - AHEAD - 1 < size:
                gather(t - AHEAD - 1)

    items = z * nx + x

    def place_of(i):
        j = i - x
        turn_of = lax.rem(j + nx, nx)
        across_x = jnp.where(j < 0, i, lax.rem(x + turn_of, nx))
        level = jnp.where(j < 0, 0, j // nx + 1)
        column = jnp.logical_and(j >= 0, turn_of == 0)
        return (z - level) * nx + across_x, column

    def pump(q):
        k, r = q // count + 1, q % count

        @pl.when(k <= z)
        def _():
            src = sp - k * nx
            arrival(src, r).wait_recv()

            @pl.when(z < nz - 1)
            def _():
                up_copy(k, r).start()

            for step in range(1, nx):
                relay(k, r, step).start()
            share(src, r).start()

    def fetch(i):
        src, column = place_of(i)

        @pl.when(jnp.logical_and(i < items, jnp.logical_not(column)))
        def _():
            for r in range(count):
                arrival(src, r).wait_recv()
                share(src, r).start()

    def take(i, slot):
        src, _ = place_of(i)
        with jax.named_scope("sharewait"):
            for r in range(count):
                share_arrival(src, r).wait_recv()
        raise_keys(src, slot, list(range(count)))
        with jax.named_scope("pump"):
            @pl.when(i > 0)
            def _():
                pump(3 + 2 * i)
                pump(4 + 2 * i)

        with jax.named_scope("fetch"):
            fetch(i + 1)

    def pass_on(r):
        for step in range(1, ny):
            other = lax.rem(y + ny - step, ny)
            y_arrival(r, other).wait_recv()
            forward(r, other).start()

    def project(r):
        with jax.named_scope(f"tokwait{r}"):
            if r == 0:
                pass_on(r)
            own_arrival(r).wait_recv()
            for step in range(1, ny):
                forward_arrival(r, lax.rem(y + ny - step, ny)).wait_recv()
        if r == 0:
            with jax.named_scope("wload2"):
                for load in loads[2:5]:
                    load.wait()
        here = part(r)
        wide = jnp.concatenate([buf[s, here] for s in range(n)], axis=1).astype(F32)
        factor = lax.rsqrt(jnp.sum(wide * wide, axis=1, keepdims=True) / (n * width) + EPSILON)
        scaled = (wide * pre[...]).astype(BF)
        scale_of[here] = scaled
        factors[here] = jnp.broadcast_to(factor, (chunk, LANES))
        flat = jnp.broadcast_to(factor, (chunk, LANES)).T[:1]
        cosine, sine = angle[: ROPE // 2, here], angle[ROPE // 2 :, here]

        def rotate(first, second):
            return jnp.concatenate(
                [first * cosine - second * sine, second * cosine + first * sine], axis=0
            )

        kv = dot(scaled, vk[...]) * factor
        kv = kv * lax.rsqrt(jnp.mean(kv * kv, axis=1, keepdims=True) + EPSILON) * kg[...]
        kvs[sp, r, :chunk] = kv.astype(BF)
        key = dot_nt(vr[...], scaled) * flat
        key = rotate(key[: ROPE // 2], key[ROPE // 2 :])
        kvs[sp, r, chunk:] = jnp.concatenate(
            [key[g * TURN : (g + 1) * TURN] for g in range(ROPE // TURN)], axis=1
        ).astype(BF)
        @pl.when(z < nz - 1)
        def _():
            up_copy(0, r).start()

        for step in range(1, nx):
            @pl.when(x + step < nx)
            def _(step=step):
                own_side(r, step).start()

        if r == 0:
            with jax.named_scope("wload5"):
                loads[5].wait()
        q = dot(scaled, vq[...]) * factor
        gains = jnp.concatenate([qg[i : i + 1] for i in range(qg.shape[0])], axis=1)
        q = q * lax.rsqrt(jnp.mean(q * q, axis=1, keepdims=True) + EPSILON) * gains
        with jax.named_scope("passon"):
            if r + 1 < count:
                pass_on(r + 1)
            else:
                pump(0)
        query = dot_nt(vut[...], q.astype(BF))
        for h in range(heads):
            p, low_half = h // 2, h % 2
            base = h * (NOPE + ROPE)
            span = slice(low_half * chunk, (low_half + 1) * chunk)
            qt[r, p, low_half * NOPE : (low_half + 1) * NOPE, span] = query[
                base : base + NOPE
            ].astype(BF)
            middle = base + NOPE + ROPE // 2
            qt[r, p, 2 * NOPE : 2 * NOPE + ROPE, span] = rotate(
                query[base + NOPE : middle], query[middle : base + NOPE + ROPE]
            ).astype(BF)

    def branch(r):
        here = part(r)
        scaled, factor = scale_of[here], factors[here, :1]
        inner = (dot(scaled, vi[...]) * factor).astype(BF).astype(F32)
        source = (dot(scaled, vs[...]) * factor).astype(BF).astype(F32)
        driven = (inner * source).astype(BF)
        ext[8 + r * chunk : 8 + (r + 1) * chunk] = driven.astype(F32)
        if r == count - 1:
            tail[...] = driven[chunk - HALO :]

            @pl.when(sp < nsp - 1)
            def _():
                halo_copy().start()
        outer[here] = (dot(scaled, vo[...]) * factor).astype(BF)

    def diagonal(r):
        with jax.named_scope(f"diag{r}"):
            raise_keys(sp, 0, [r])
            units([(r, p, 0) for p in range(pairs)], True)

    for r in range(count):
        project(r)
    with jax.named_scope("wload6"):
        for load in loads[6:9]:
            load.wait()
    with jax.named_scope("pump1"):
        pump(1)
    for r in range(count - 1, -1, -1):
        with jax.named_scope("branch"):
            branch(r)
    with jax.named_scope("prefetch"):
        fetch(0)
        pump(2)
        pump(3)
    for r in range(count):
        diagonal(r)
    with jax.named_scope("pump4"):
        pump(4)

    wave = jnp.minimum(items, WAVE)

    def whole(i, carry):
        take(i, 0)
        with jax.named_scope("units"):
          units([(c, p, 0) for c in range(count) for p in range(pairs)], False)
        return carry

    lax.fori_loop(0, items - wave, whole, 0)

    def ready(w, carry):
        take(items - wave + w, w)
        return carry

    lax.fori_loop(0, wave, ready, 0)

    @pl.when(sp == 0)
    def _():
        ext[:8] = jnp.zeros((8, ext.shape[1]), F32)

    @pl.when(sp > 0)
    def _():
        remote(tail, halo, h_s.at[0], h_r.at[0], tp=partner).wait_recv()
        ext[:8] = halo[...].astype(F32)[HALO - 8 :]

    def product(r, dest):
        columns = pl.ds(pl.multiple_of(dest * width, width), width)
        return (
            dot(att[part(r), : heads * VDIM], va[:, columns])
            + dot(att[part(r), heads * VDIM :], vc[:, columns])
        ).astype(BF)

    def to_partner(r, step):
        return remote(
            away.at[step, part(r)], pin.at[step, part(r)], a_s.at[r, step], a_r.at[r, step], tp=partner
        )

    def across(r, step):
        to = lax.rem(y + step, ny) * 2 + core
        return remote(
            ysend.at[step, part(r)], yin.at[step, part(r)], b_s.at[r, step], b_r.at[r, step], tp=to
        )

    def home(r):
        return remote(peer.at[part(r)], pown.at[part(r)], p_s.at[r], p_r.at[r], tp=partner)

    def squares(r, step):
        return remote(
            sq.at[r], sqin.at[step, r], q_s.at[r, step], q_r.at[r, step], tp=lax.rem(tp + step, n)
        )

    for load in loads[9:]:
        load.wait()

    def send_on(c):
        for step in range(1, ny):
            with jax.named_scope("partnerwait"):
                to_partner(c, step).wait_recv()
            ysend[step, part(c)] = (
                mine[step, part(c)].astype(F32) + pin[step, part(c)].astype(F32)
            ).astype(BF)
            across(c, step).start()

    for c in range(count):
        @pl.when(items >= WAVE)
        def _(c=c):
            with jax.named_scope("lastunits"):
                units([(c, p, w) for w in range(WAVE) for p in range(pairs)], False)

        @pl.when(items < WAVE)
        def _(c=c):
            def last(w, carry):
                units([(c, p, w) for p in range(pairs)], False)
                return carry

            lax.fori_loop(0, items, last, 0)

        for p in range(pairs):
            value = acc[c, p] / low[c, p]
            both = jnp.concatenate([value[:, :chunk], value[:, chunk:]], axis=0)
            att[part(c), p * LANES : (p + 1) * LANES] = both.T.astype(BF)
            log = top[c, p] * math.log(2.0) + jnp.log(low[c, p])
            logs[2 * p : 2 * p + 1, part(c)] = log[:, :chunk]
            logs[2 * p + 1 : 2 * p + 2, part(c)] = log[:, chunk:]
        conv = jnp.zeros((chunk, ext.shape[1]), F32)
        for index in range(TAPS):
            start = 8 + c * chunk - (TAPS - 1) + index
            conv = conv + taps[index : index + 1].astype(F32) * ext[start : start + chunk]
        att[part(c), heads * VDIM :] = (outer[part(c)].astype(F32) * conv).astype(BF)
        for step in range(1, ny):
            dest = lax.rem(y + step, ny) * 2
            away[step, part(c)] = product(c, dest + 1 - core)
            to_partner(c, step).start()
            mine[step, part(c)] = product(c, dest + core)
        peer[part(c)] = product(c, partner)
        home(c).start()
        total[part(c)] = product(c, tp).astype(F32)
        send_on(c)
    for r in range(count):
        own_copy(r).wait_send()
        for step in range(1, ny):
            y_copy(r, step).wait_send()
            forward(r, lax.rem(y + step, ny)).wait_send()
        for step in range(1, nx):
            @pl.when(x + step < nx)
            def _(step=step, r=r):
                own_side(r, step).wait_send()

    @pl.when(sp < nsp - 1)
    def _():
        halo_copy().wait_send()

    def sent(i, carry):
        src, _ = place_of(i)
        for r in range(count):
            share(src, r).wait_send()
        return carry

    lax.fori_loop(0, items, sent, 0)

    def relayed(k, carry):
        for r in range(count):
            for step in range(1, nx):
                relay(k, r, step).wait_send()
        return carry

    lax.fori_loop(1, z + 1, relayed, 0)

    @pl.when(z < nz - 1)
    def _():
        def raised(k, carry):
            for r in range(count):
                up_copy(k, r).wait_send()
            return carry

        lax.fori_loop(0, z + 1, raised, 0)

    for r in range(count):
        with jax.named_scope("homewait"):
            home(r).wait_recv()
        value = total[part(r)] + pown[part(r)].astype(F32)
        for step in range(1, ny):
            with jax.named_scope("acrosswait"):
                across(r, step).wait_recv()
            value = value + yin[step, part(r)].astype(F32)
        total[part(r)] = value
        sums = jnp.sum(value * value, axis=1, keepdims=True)
        sq[r] = jnp.broadcast_to(sums, (chunk, LANES)).T[:8]
        for step in range(1, n):
            squares(r, step).start()
    for r in range(count):
        whole_sum = sq[r]
        for step in range(1, n):
            with jax.named_scope("sqwait"):
                squares(r, step).wait_recv()
            whole_sum = whole_sum + sqin[step, r]
        with jax.named_scope("outs"):
          scale = lax.rsqrt(whole_sum / (n * width) + EPSILON)
          column = jnp.broadcast_to(scale[:1], (LANES, chunk)).T[:, :1]
          out[part(r)] = (total[part(r)] * column * gain[...]).astype(BF)

    with jax.named_scope("endsend"):
     for r in range(count):
        home(r).wait_send()
        for step in range(1, ny):
            to_partner(r, step).wait_send()
            across(r, step).wait_send()
        for step in range(1, n):
            squares(r, step).wait_send()


DMA = pltpu.SemaphoreType.DMA


def angles(tokens):
    freqs = np.float32(THETA) ** (-np.arange(0, ROPE, 2, dtype=np.float32) / np.float32(ROPE))
    phase = freqs.astype(np.float32)[:, None] * np.arange(tokens, dtype=np.float32)[None, :]
    phase = phase.astype(np.float64)
    return np.concatenate([np.cos(phase), np.sin(phase)], axis=0).astype(np.float32)


def body(
    nsp, ntp,
    tokens, pre_gain, outer_gate_weight, inner_gate_weight, source_weight, conv_taps,
    q_down_weight, q_norm_gain, q_up_weight, kv_down_weight, rope_key_weight, kv_norm_gain,
    kv_up_weight, attn_out_weight, conv_out_weight, post_gain,
):
    rows, width = tokens.shape
    ny = ntp // 2
    nx = ny if nsp % ny == 0 else 1
    nz = nsp // nx
    chunk = LANES
    count = rows // chunk
    q_rank, rank = q_down_weight.shape[1], kv_down_weight.shape[1]
    channels = outer_gate_weight.shape[1]
    heads = q_up_weight.shape[1] // (NOPE + ROPE)
    pairs = heads // 2
    struct = jax.ShapeDtypeStruct
    v = pltpu.VMEM
    whole = pl.BlockSpec(memory_space=pltpu.VMEM)
    anywhere = pl.BlockSpec(memory_space=pl.ANY)
    rope_turned = rope_key_weight.T
    weights = (
        outer_gate_weight, inner_gate_weight, source_weight, q_down_weight, kv_down_weight,
        rope_turned, q_up_weight, kv_up_weight, attn_out_weight, conv_out_weight,
    )
    block = (ny, rows, width)
    return pl.pallas_call(
        functools.partial(layer_kernel, nz, nx, ntp, chunk, heads),
        out_shape=[v((rows, width), BF), v((heads, rows), F32)],
        in_specs=[anywhere] + [whole] * 5 + [anywhere] * (1 + len(weights)),
        out_specs=[whole] * 2,
        scratch_shapes=[v((ntp, rows, width), BF)]
        + [v(w.shape, BF) for w in weights]
        + [
            v((ROPE, rows), F32),
            v(q_up_weight.shape[::-1], BF),
            v((rank, heads * NOPE), BF), v((heads * VDIM, rank), BF),
            v((count, pairs, 2 * LANES, 2 * chunk), BF),
            v((nsp, count, chunk + TURN, rank), BF),
            v((WAVE, rows, heads * NOPE), BF), v((WAVE, rows, LANES), BF),
            v((WAVE, heads * VDIM, rows), BF),
            v((AHEAD + 2, rows, 2 * chunk), F32),
            v((count, pairs, VDIM, 2 * chunk), F32),
            v((count, pairs, 1, 2 * chunk), F32), v((count, pairs, 1, 2 * chunk), F32),
            v((rows, ntp * width), BF), v((rows, LANES), F32),
            v((rows, channels), BF), v((8 + rows, channels), F32),
            v((HALO, channels), BF), v((HALO, channels), BF),
            v((rows, heads * VDIM + channels), BF),
        ]
        + [v(block, BF)] * 5
        + [
            v((rows, width), BF), v((rows, width), BF), v((rows, width), F32),
            v((count, 8, chunk), F32), v((ntp, count, 8, chunk), F32),
            DMA((count,)), DMA((11,)), DMA((count,)), DMA((count,)),
            DMA((count, ny)), DMA((count, ny)), DMA((count, ny)), DMA((count, ny)),
            DMA((nz, count)), DMA((count, nx)), DMA((nz, count, nx)),
            DMA((nsp, count)), DMA((nsp, count)), DMA((nsp, count)), DMA((1,)), DMA((1,)),
            DMA((count, ny)), DMA((count, ny)), DMA((count, ny)), DMA((count, ny)),
            DMA((count,)), DMA((count,)), DMA((count, ntp)), DMA((count, ntp)),
        ],
        compiler_params=pltpu.CompilerParams(
            collective_id=0, has_side_effects=True, vmem_limit_bytes=60 * 1024 * 1024
        ),
        name="layer",
    )(
        tokens, pre_gain[None], q_norm_gain.reshape(-1, LANES), kv_norm_gain[None],
        post_gain[None], conv_taps, jnp.asarray(angles(nsp * rows)), *weights,
    )


def solution(mesh):
    placed = (
        P("sp", "tp"), P(), P(None, "tp"), P(None, "tp"), P(None, "tp"), P(None, "tp"), P(), P(),
        P(None, "tp"), P(), P(), P(), P(None, "tp"), P("tp", None), P("tp", None), P("tp"),
    )
    return jax.shard_map(
        functools.partial(body, mesh.shape["sp"], mesh.shape["tp"]),
        mesh=mesh,
        in_specs=placed,
        out_specs=(P("sp", "tp"), P("tp", "sp")),
        check_vma=False,
    )
```

```python
import functools
import math

import jax
import jax.numpy as jnp
import numpy as np
from jax import lax
from jax.experimental import pallas as pl
from jax.experimental.pallas import tpu as pltpu
from jax.sharding import PartitionSpec as P

NOPE = 64
ROPE = 32
VDIM = 64
TAPS = 3
LANES = 128
HALO = 16
TURN = 8
AHEAD = 2
WAVE = 3

EPSILON = 1e-06
THETA = 500000.0
NEGATIVE = -1e30
MESH = pl.DeviceIdType.MESH
BF = jnp.bfloat16
F32 = jnp.float32


def remote(src, dst, send, recv, **where):
    return pltpu.make_async_remote_copy(
        src_ref=src, dst_ref=dst, send_sem=send, recv_sem=recv, device_id=where, device_id_type=MESH
    )


def dot(a, b):
    return jnp.dot(a, b, preferred_element_type=F32)


def dot_nt(a, b):
    return lax.dot_general(a, b, (((1,), (1,)), ((), ())), preferred_element_type=F32)


def layer_kernel(
    nz, nx, n, chunk, heads,
    tok, pre, qg, kg, gain, taps, table, wo, wi, ws, wq, wk, wr, wu, wkv, wa, wc,
    out, logs,
    buf, vo, vi, vs, vq, vk, vr, vu, vkv, va, vc, angle,
    vut, upk, upvt, qt, kvs, kn, turn, vt, sbuf, acc, top, low,
    scale_of, factors, outer, ext, tail, halo, att,
    away, mine, pin, ysend, yin, peer, pown, total, sq, sqin,
    t_s, w_s, own_s, own_r, y_s, y_r, f_s, f_r,
    z_s, o_s, x_s, i_r, d_s, d_r, h_s, h_r,
    a_s, a_r, b_s, b_r, p_s, p_r, q_s, q_r,
):
    sp, tp = lax.axis_index("sp"), lax.axis_index("tp")
    nsp = nz * nx
    z, x = sp // nx, lax.rem(sp, nx)
    ny = n // 2
    y, core = tp // 2, lax.rem(tp, 2)
    partner = tp + 1 - 2 * core
    rows, width = tok.shape
    count = rows // chunk
    pairs = heads // 2
    rank = wkv.shape[0]
    factor2 = (NOPE + ROPE) ** (-0.5) * math.log2(math.e)
    side = pl.ds(pl.multiple_of(core * (rank // 2), LANES), rank // 2)

    def part(r):
        return pl.ds(r * chunk, chunk)

    tokens = [
        pltpu.make_async_copy(tok.at[part(r)], buf.at[tp, part(r)], t_s.at[r]) for r in range(count)
    ]
    place = pl.ds(pl.multiple_of(sp * rows, LANES), rows)
    pairs_of = (
        (wu, vu), (wkv, vkv), (table.at[:, place], angle), (wk, vk), (wr, vr), (wq, vq),
        (wi, vi), (ws, vs), (wo, vo), (wa, va), (wc, vc),
    )
    loads = [pltpu.make_async_copy(a, b, w_s.at[i]) for i, (a, b) in enumerate(pairs_of)]
    for token in tokens:
        token.start()

    barrier = pltpu.get_barrier_semaphore()

    def greet(**where):
        pl.semaphore_signal(barrier, inc=1, device_id=where, device_id_type=MESH)

    for step in range(1, n):
        greet(tp=lax.rem(tp + step, n))
    greet(sp=lax.rem(z + 1, nz) * nx + x)
    greet(sp=lax.rem(z + nz - 1, nz) * nx + x)
    for step in range(1, nx):
        greet(sp=z * nx + lax.rem(x + step, nx))
    greet(sp=lax.rem(sp + 1, nsp))
    greet(sp=lax.rem(sp + nsp - 1, nsp))
    for load in loads:
        load.start()
    with jax.named_scope("barrier"):
        pl.semaphore_wait(barrier, n - 1 + 2 + nx - 1 + 2)

    def y_copy(r, step):
        to = lax.rem(y + step, ny) * 2 + core
        here = buf.at[tp, part(r)]
        return remote(here, here, y_s.at[step - 1], y_r.at[r, step - 1], tp=to)

    def y_other(step):
        return lax.rem(y + ny - step, ny)

    def y_arrival(r, step):
        here = buf.at[y_other(step) * 2 + core, part(r)]
        return remote(here, here, y_s.at[step - 1], y_r.at[r, step - 1], tp=partner)

    def own_copy(r):
        here = buf.at[tp, part(r)]
        return remote(here, here, own_s.at[0], own_r.at[r], tp=partner)

    def own_arrival(r):
        here = buf.at[partner, part(r)]
        return remote(here, here, own_s.at[0], own_r.at[r], tp=partner)

    def forward(r, step):
        here = buf.at[y_other(step) * 2 + core, part(r)]
        return remote(here, here, f_s.at[step - 1], f_r.at[r, step - 1], tp=partner)

    def forward_arrival(r, step):
        here = buf.at[y_other(step) * 2 + 1 - core, part(r)]
        return remote(here, here, f_s.at[step - 1], f_r.at[r, step - 1], tp=partner)

    def tokens_sent():
        here = buf.at[tp]
        remote(here, here, own_s.at[0], own_r.at[0], tp=partner).wait_send()
        for step in range(1, ny):
            remote(here, here, y_s.at[step - 1], own_r.at[0], tp=partner).wait_send()
            remote(here, here, f_s.at[step - 1], own_r.at[0], tp=partner).wait_send()

    def piece(src, r):
        return kvs.at[src, r, :, side]

    def up_copy(k, r):
        src = sp - k * nx
        return remote(piece(src, r), piece(src, r), z_s.at[k], i_r.at[src, r], sp=sp + nx)

    def own_side(r, step):
        to = z * nx + lax.rem(x + step, nx)
        return remote(piece(sp, r), piece(sp, r), o_s.at[step - 1], i_r.at[sp, r], sp=to)

    def relay(k, r, step):
        src = sp - k * nx
        to = z * nx + lax.rem(x + step, nx)
        return remote(piece(src, r), piece(src, r), x_s.at[k - 1, step - 1], i_r.at[src, r], sp=to)

    def arrival(src, r):
        return remote(piece(src, r), piece(src, r), z_s.at[0], i_r.at[src, r], tp=partner)

    def share(src, r):
        return remote(piece(src, r), piece(src, r), d_s.at[src], d_r.at[src], tp=partner)

    def share_arrival(src):
        other = pl.ds(pl.multiple_of((1 - core) * (rank // 2), LANES), rank // 2)
        here = kvs.at[src, :, :, other]
        return remote(here, here, d_s.at[src], d_r.at[src], tp=partner)

    def block_sent(sem):
        here = kvs.at[sp, :, :, side]
        remote(here, here, sem, d_r.at[0], tp=partner).wait_send()

    def halo_copy():
        return remote(tail, halo, h_s.at[0], h_r.at[0], sp=sp + 1)

    with jax.named_scope("sendtok"):
        for r in range(count):
            tokens[r].wait()
            for step in range(1, ny):
                y_copy(r, step).start()
            own_copy(r).start()

    with jax.named_scope("wturn"):
        qt[...] = jnp.zeros_like(qt)
        loads[0].wait()
        vut[...] = vu[...].T
    with jax.named_scope("wload1"):
        loads[1].wait()
    for p in range(pairs):
        first, second = 2 * p * LANES, (2 * p + 1) * LANES
        upk[:, p * LANES : (p + 1) * LANES] = jnp.concatenate(
            [vkv[:, first : first + NOPE], vkv[:, second : second + NOPE]], axis=1
        )
    turned = vkv[...].T
    for h in range(heads):
        upvt[h * VDIM : (h + 1) * VDIM] = turned[h * LANES + NOPE : (h + 1) * LANES]

    def raise_keys(src, slot, span):
        here = pl.ds(span[0] * chunk, len(span) * chunk)

        def latent():
            return jnp.concatenate([kvs[src, r, :chunk] for r in span], axis=0)

        def keys(start, stop):
            kn[slot, here, start:stop] = dot(latent(), upk[:, start:stop]).astype(BF)

        def values():
            vt[slot, :, here] = dot_nt(upvt[...], latent()).astype(BF)

        def turns(r):
            packed = kvs[src, r, chunk:].astype(F32)
            tall = jnp.concatenate(
                [packed[:, g * LANES : (g + 1) * LANES] for g in range(ROPE // TURN)]
                + [jnp.zeros((LANES - ROPE, LANES), F32)],
                axis=0,
            )
            turn[slot, part(r)] = tall.T.astype(BF)

        wide = heads * NOPE
        cut = min(wide, 2 * LANES)
        parts = [functools.partial(keys, s, s + cut) for s in range(0, wide, cut)]
        return parts + [values] + [functools.partial(turns, r) for r in span]

    def do(parts):
        for one in parts:
            one()

    def units(todo, diagonal, parts=()):
        peaks, ready = {}, {}
        size = len(todo)

        def keys(c):
            return (c + 1) * chunk if diagonal else rows

        def score(i):
            c, p, slot = todo[i]
            k = keys(c)
            left = jnp.concatenate(
                [kn[slot, :k, p * LANES : (p + 1) * LANES], turn[slot, :k]], axis=1
            )
            s = dot(left, qt[c, p])
            if diagonal:
                last = s[k - chunk :]
                key = lax.broadcasted_iota(jnp.int32, last.shape, 0)
                query = lax.rem(lax.broadcasted_iota(jnp.int32, last.shape, 1), chunk)
                last = jnp.where(key <= query, last, NEGATIVE)
                s = last if k == chunk else jnp.concatenate([s[: k - chunk], last], axis=0)
            sbuf[i % (AHEAD + 2), :k] = s
            peaks[i] = jnp.max(s, axis=0, keepdims=True) * factor2

        def soften(i):
            c, p, slot = todo[i]
            peak = peaks.pop(i)
            shrink = None
            if not diagonal:
                before = top[c, p]
                peak = jnp.maximum(before, peak)
                shrink = jnp.exp2(before - peak)
            w = jnp.exp2(sbuf[i % (AHEAD + 2), : keys(c)] * factor2 - peak)
            sums = jnp.sum(w, axis=0, keepdims=True)
            low[c, p] = sums if diagonal else low[c, p] * shrink + sums
            top[c, p] = peak
            ready[i] = (w.astype(BF), shrink)

        def gather(i):
            c, p, slot = todo[i]
            w, shrink = ready.pop(i)
            o = dot(vt[slot, p * LANES : (p + 1) * LANES, : keys(c)], w)
            o = jnp.concatenate([o[:VDIM, :chunk], o[VDIM:, chunk:]], axis=1)
            acc[c, p] = o if diagonal else acc[c, p] * shrink + o

        parts = list(parts)
        for t in range(size + AHEAD + 1):
            if t < size:
                score(t)
            if parts:
                parts.pop(0)()
            if 0 <= t - AHEAD < size:
                soften(t - AHEAD)
            if 0 <= t - AHEAD - 1 < size:
                gather(t - AHEAD - 1)
        do(parts)

    items = z * nx + x

    def place_of(i):
        j = i - x - 1
        block, spot = (j + nx) // nx - 1, lax.rem(j + nx, nx)
        late = block >= z - 1
        column = jnp.where(late, False, spot == 0)
        step = jnp.where(late, spot + 1, spot)
        level = jnp.where(late, z, jnp.where(spot == 0, block + 2, block + 1))
        column = jnp.logical_or(j == -1, column)
        step = jnp.where(j == -1, 0, step)
        level = jnp.where(j == -1, 1, level)
        level = jnp.where(j < -1, 0, level)
        column = jnp.logical_and(j >= -1, column)
        across_x = jnp.where(j < -1, i, lax.rem(x + step, nx))
        return (z - level) * nx + across_x, column

    def pump(q):
        k, r = q // count + 1, q % count

        @pl.when(k <= z)
        def _():
            src = sp - k * nx
            arrival(src, r).wait_recv()

            @pl.when(z < nz - 1)
            def _():
                up_copy(k, r).start()

            for step in range(1, nx):
                relay(k, r, step).start()
            share(src, r).start()

    def fetch(i):
        src, column = place_of(i)

        @pl.when(jnp.logical_and(i < items, jnp.logical_not(column)))
        def _():
            for r in range(count):
                arrival(src, r).wait_recv()
                share(src, r).start()

    def shared(i):
        src, _ = place_of(i)
        with jax.named_scope("sharewait"):
            share_arrival(src).wait_recv()

    def prepare(i):
        with jax.named_scope("pump"):
            pump(5 + 2 * i)
            pump(6 + 2 * i)
        with jax.named_scope("fetch"):
            fetch(i + 2)

    def pass_on(r):
        for step in range(1, ny):
            y_arrival(r, step).wait_recv()
            forward(r, step).start()

    def project(r):
        with jax.named_scope(f"tokwait{r}"):
            if r == 0:
                pass_on(r)
            own_arrival(r).wait_recv()
            for step in range(1, ny):
                forward_arrival(r, step).wait_recv()
        if r == 0:
            with jax.named_scope("wload2"):
                for load in loads[2:5]:
                    load.wait()
        here = part(r)
        wide = jnp.concatenate([buf[s, here] for s in range(n)], axis=1).astype(F32)
        factor = lax.rsqrt(jnp.sum(wide * wide, axis=1, keepdims=True) / (n * width) + EPSILON)
        scaled = (wide * pre[...]).astype(BF)
        scale_of[here] = scaled
        factors[here] = jnp.broadcast_to(factor, (chunk, LANES))
        flat = jnp.broadcast_to(factor, (chunk, LANES)).T[:1]
        cosine, sine = angle[: ROPE // 2, here], angle[ROPE // 2 :, here]

        def rotate(first, second):
            return jnp.concatenate(
                [first * cosine - second * sine, second * cosine + first * sine], axis=0
            )

        kv = dot(scaled, vk[...]) * factor
        kv = kv * lax.rsqrt(jnp.mean(kv * kv, axis=1, keepdims=True) + EPSILON) * kg[...]
        kvs[sp, r, :chunk] = kv.astype(BF)
        key = dot_nt(vr[...], scaled) * flat
        key = rotate(key[: ROPE // 2], key[ROPE // 2 :])
        kvs[sp, r, chunk:] = jnp.concatenate(
            [key[g * TURN : (g + 1) * TURN] for g in range(ROPE // TURN)], axis=1
        ).astype(BF)
        @pl.when(z < nz - 1)
        def _():
            up_copy(0, r).start()

        for step in range(1, nx):
            @pl.when(x + step < nx)
            def _(step=step):
                own_side(r, step).start()

        if r == 0:
            with jax.named_scope("wload5"):
                loads[5].wait()
        q = dot(scaled, vq[...]) * factor
        gains = jnp.concatenate([qg[i : i + 1] for i in range(qg.shape[0])], axis=1)
        q = q * lax.rsqrt(jnp.mean(q * q, axis=1, keepdims=True) + EPSILON) * gains
        with jax.named_scope("passon"):
            if r + 1 < count:
                pass_on(r + 1)
            else:
                pump(0)
        query = dot_nt(vut[...], q.astype(BF))
        for h in range(heads):
            p, low_half = h // 2, h % 2
            base = h * (NOPE + ROPE)
            span = slice(low_half * chunk, (low_half + 1) * chunk)
            qt[r, p, low_half * NOPE : (low_half + 1) * NOPE, span] = query[
                base : base + NOPE
            ].astype(BF)
            middle = base + NOPE + ROPE // 2
            qt[r, p, 2 * NOPE : 2 * NOPE + ROPE, span] = rotate(
                query[base + NOPE : middle], query[middle : base + NOPE + ROPE]
            ).astype(BF)

    def branch(r):
        here = part(r)
        scaled, factor = scale_of[here], factors[here, :1]
        inner = (dot(scaled, vi[...]) * factor).astype(BF).astype(F32)
        source = (dot(scaled, vs[...]) * factor).astype(BF).astype(F32)
        driven = (inner * source).astype(BF)
        ext[8 + r * chunk : 8 + (r + 1) * chunk] = driven.astype(F32)
        if r == count - 1:
            tail[...] = driven[chunk - HALO :]

            @pl.when(sp < nsp - 1)
            def _():
                halo_copy().start()
        outer[here] = (dot(scaled, vo[...]) * factor).astype(BF)

    for r in range(count):
        project(r)
    with jax.named_scope("wload6"):
        for load in loads[6:9]:
            load.wait()
    with jax.named_scope("pump1"):
        pump(1)
    for r in range(count - 1, -1, -1):
        with jax.named_scope("branch"):
            branch(r)
    with jax.named_scope("prefetch"):
        fetch(0)
        fetch(1)
        pump(2)
        pump(3)
    with jax.named_scope("diag"):
        do(raise_keys(sp, 0, list(range(count))))
        units([(r, p, 0) for r in range(count) for p in range(pairs)], True)
    with jax.named_scope("pump4"):
        pump(4)

    everything = list(range(count))
    many = items >= WAVE

    @pl.when(many)
    def _():
        shared(0)
        with jax.named_scope("raise0"):
            do(raise_keys(place_of(0)[0], 0, everything))

        def whole(i, carry):
            prepare(i)
            shared(i + 1)
            with jax.named_scope("units"):
                units(
                    [(c, p, 0) for c in everything for p in range(pairs)], False,
                    raise_keys(place_of(i + 1)[0], 1, everything),
                )
                for old in (kn, vt, turn):
                    old[0] = old[1]
            return carry

        lax.fori_loop(0, items - WAVE, whole, 0)
        for w in range(WAVE - 1):
            prepare(items - WAVE + w)
            shared(items - WAVE + w + 1)
            with jax.named_scope("waveunits"):
                units(
                    [(0, p, w) for p in range(pairs)], False,
                    raise_keys(place_of(items - WAVE + w + 1)[0], w + 1, everything),
                )
        with jax.named_scope("waveunits"):
            units([(0, p, WAVE - 1) for p in range(pairs)], False)

    @pl.when(jnp.logical_not(many))
    def _():
        def ready(w, carry):
            prepare(w)
            shared(w)
            do(raise_keys(place_of(w)[0], w, everything))
            return carry

        lax.fori_loop(0, items, ready, 0)

    @pl.when(sp == 0)
    def _():
        ext[:8] = jnp.zeros((8, ext.shape[1]), F32)

    @pl.when(sp > 0)
    def _():
        remote(tail, halo, h_s.at[0], h_r.at[0], tp=partner).wait_recv()
        ext[:8] = halo[...].astype(F32)[HALO - 8 :]

    def product(r, dest):
        columns = pl.ds(pl.multiple_of(dest * width, width), width)
        return (
            dot(att[part(r), : heads * VDIM], va[:, columns])
            + dot(att[part(r), heads * VDIM :], vc[:, columns])
        ).astype(BF)

    def to_partner(r, step):
        return remote(
            away.at[step, part(r)], pin.at[step, part(r)], a_s.at[step - 1], a_r.at[r, step - 1], tp=partner
        )

    def across(r, step):
        to = lax.rem(y + step, ny) * 2 + core
        return remote(
            ysend.at[step, part(r)], yin.at[step, part(r)], b_s.at[step - 1], b_r.at[r, step - 1], tp=to
        )

    def home(r):
        return remote(peer.at[part(r)], pown.at[part(r)], p_s.at[0], p_r.at[r], tp=partner)

    def squares(r, step):
        return remote(
            sq.at[r], sqin.at[step, r], q_s.at[step - 1], q_r.at[r, step - 1], tp=lax.rem(tp + step, n)
        )

    for load in loads[9:]:
        load.wait()

    def send_on(c):
        for step in range(1, ny):
            with jax.named_scope("partnerwait"):
                to_partner(c, step).wait_recv()
            ysend[step, part(c)] = (
                mine[step, part(c)].astype(F32) + pin[step, part(c)].astype(F32)
            ).astype(BF)
            across(c, step).start()

    for c in range(count):
        if c > 0:
            @pl.when(many)
            def _(c=c):
                with jax.named_scope("lastunits"):
                    units([(c, p, w) for w in range(WAVE) for p in range(pairs)], False)

        @pl.when(jnp.logical_not(many))
        def _(c=c):
            def last(w, carry):
                units([(c, p, w) for p in range(pairs)], False)
                return carry

            lax.fori_loop(0, items, last, 0)

        for p in range(pairs):
            value = acc[c, p] / low[c, p]
            both = jnp.concatenate([value[:, :chunk], value[:, chunk:]], axis=0)
            att[part(c), p * LANES : (p + 1) * LANES] = both.T.astype(BF)
            log = top[c, p] * math.log(2.0) + jnp.log(low[c, p])
            logs[2 * p : 2 * p + 1, part(c)] = log[:, :chunk]
            logs[2 * p + 1 : 2 * p + 2, part(c)] = log[:, chunk:]
        conv = jnp.zeros((chunk, ext.shape[1]), F32)
        for index in range(TAPS):
            start = 8 + c * chunk - (TAPS - 1) + index
            conv = conv + taps[index : index + 1].astype(F32) * ext[start : start + chunk]
        att[part(c), heads * VDIM :] = (outer[part(c)].astype(F32) * conv).astype(BF)
        for step in range(1, ny):
            dest = lax.rem(y + step, ny) * 2
            away[step, part(c)] = product(c, dest + 1 - core)
            to_partner(c, step).start()
            mine[step, part(c)] = product(c, dest + core)
        peer[part(c)] = product(c, partner)
        home(c).start()
        total[part(c)] = product(c, tp).astype(F32)
        send_on(c)
    tokens_sent()
    for step in range(1, nx):
        @pl.when(x + step < nx)
        def _(step=step):
            block_sent(o_s.at[step - 1])

    @pl.when(sp < nsp - 1)
    def _():
        halo_copy().wait_send()

    def sent(i, carry):
        block_sent(d_s.at[place_of(i)[0]])
        return carry

    lax.fori_loop(0, items, sent, 0)

    def relayed(k, carry):
        for step in range(1, nx):
            block_sent(x_s.at[k - 1, step - 1])
        return carry

    lax.fori_loop(1, z + 1, relayed, 0)

    @pl.when(z < nz - 1)
    def _():
        def raised(k, carry):
            block_sent(z_s.at[k])
            return carry

        lax.fori_loop(0, z + 1, raised, 0)

    for r in range(count):
        with jax.named_scope("homewait"):
            home(r).wait_recv()
        value = total[part(r)] + pown[part(r)].astype(F32)
        for step in range(1, ny):
            with jax.named_scope("acrosswait"):
                across(r, step).wait_recv()
            value = value + yin[step, part(r)].astype(F32)
        total[part(r)] = value
        sums = jnp.sum(value * value, axis=1, keepdims=True)
        sq[r] = jnp.broadcast_to(sums, (chunk, LANES)).T[:8]
        for step in range(1, n):
            squares(r, step).start()
    for r in range(count):
        whole_sum = sq[r]
        for step in range(1, n):
            with jax.named_scope("sqwait"):
                squares(r, step).wait_recv()
            whole_sum = whole_sum + sqin[step, r]
        with jax.named_scope("outs"):
          scale = lax.rsqrt(whole_sum / (n * width) + EPSILON)
          column = jnp.broadcast_to(scale[:1], (LANES, chunk)).T[:, :1]
          out[part(r)] = (total[part(r)] * column * gain[...]).astype(BF)

    remote(peer, pown, p_s.at[0], p_r.at[0], tp=partner).wait_send()
    for step in range(1, ny):
        remote(peer, pown, a_s.at[step - 1], p_r.at[0], tp=partner).wait_send()
        remote(peer, pown, b_s.at[step - 1], p_r.at[0], tp=partner).wait_send()
    for step in range(1, n):
        remote(sq, sqin.at[step], q_s.at[step - 1], p_r.at[0], tp=partner).wait_send()


DMA = pltpu.SemaphoreType.DMA


def angles(tokens):
    freqs = np.float32(THETA) ** (-np.arange(0, ROPE, 2, dtype=np.float32) / np.float32(ROPE))
    phase = freqs.astype(np.float32)[:, None] * np.arange(tokens, dtype=np.float32)[None, :]
    phase = phase.astype(np.float64)
    return np.concatenate([np.cos(phase), np.sin(phase)], axis=0).astype(np.float32)


def body(
    nsp, ntp,
    tokens, pre_gain, outer_gate_weight, inner_gate_weight, source_weight, conv_taps,
    q_down_weight, q_norm_gain, q_up_weight, kv_down_weight, rope_key_weight, kv_norm_gain,
    kv_up_weight, attn_out_weight, conv_out_weight, post_gain,
):
    rows, width = tokens.shape
    ny = ntp // 2
    nx = ny if nsp % ny == 0 else 1
    nz = nsp // nx
    chunk = LANES
    count = rows // chunk
    q_rank, rank = q_down_weight.shape[1], kv_down_weight.shape[1]
    channels = outer_gate_weight.shape[1]
    heads = q_up_weight.shape[1] // (NOPE + ROPE)
    pairs = heads // 2
    struct = jax.ShapeDtypeStruct
    v = pltpu.VMEM
    whole = pl.BlockSpec(memory_space=pltpu.VMEM)
    anywhere = pl.BlockSpec(memory_space=pl.ANY)
    rope_turned = rope_key_weight.T
    weights = (
        outer_gate_weight, inner_gate_weight, source_weight, q_down_weight, kv_down_weight,
        rope_turned, q_up_weight, kv_up_weight, attn_out_weight, conv_out_weight,
    )
    block = (ny, rows, width)
    return pl.pallas_call(
        functools.partial(layer_kernel, nz, nx, ntp, chunk, heads),
        out_shape=[v((rows, width), BF), v((heads, rows), F32)],
        in_specs=[anywhere] + [whole] * 5 + [anywhere] * (1 + len(weights)),
        out_specs=[whole] * 2,
        scratch_shapes=[v((ntp, rows, width), BF)]
        + [v(w.shape, BF) for w in weights]
        + [
            v((ROPE, rows), F32),
            v(q_up_weight.shape[::-1], BF),
            v((rank, heads * NOPE), BF), v((heads * VDIM, rank), BF),
            v((count, pairs, 2 * LANES, 2 * chunk), BF),
            v((nsp, count, chunk + TURN, rank), BF),
            v((WAVE, rows, heads * NOPE), BF), v((WAVE, rows, LANES), BF),
            v((WAVE, heads * VDIM, rows), BF),
            v((AHEAD + 2, rows, 2 * chunk), F32),
            v((count, pairs, VDIM, 2 * chunk), F32),
            v((count, pairs, 1, 2 * chunk), F32), v((count, pairs, 1, 2 * chunk), F32),
            v((rows, ntp * width), BF), v((rows, LANES), F32),
            v((rows, channels), BF), v((8 + rows, channels), F32),
            v((HALO, channels), BF), v((HALO, channels), BF),
            v((rows, heads * VDIM + channels), BF),
        ]
        + [v(block, BF)] * 5
        + [
            v((rows, width), BF), v((rows, width), BF), v((rows, width), F32),
            v((count, 8, chunk), F32), v((ntp, count, 8, chunk), F32),
            DMA((count,)), DMA((11,)), DMA((1,)), DMA((count,)),
            DMA((ny - 1,)), DMA((count, ny - 1)), DMA((ny - 1,)), DMA((count, ny - 1)),
            DMA((nz,)), DMA((nx - 1,)), DMA((nz - 1, nx - 1)),
            DMA((nsp, count)), DMA((nsp,)), DMA((nsp,)), DMA((1,)), DMA((1,)),
            DMA((ny - 1,)), DMA((count, ny - 1)), DMA((ny - 1,)), DMA((count, ny - 1)),
            DMA((1,)), DMA((count,)), DMA((ntp - 1,)), DMA((count, ntp - 1)),
        ],
        compiler_params=pltpu.CompilerParams(
            collective_id=0, has_side_effects=True, vmem_limit_bytes=60 * 1024 * 1024
        ),
        name="layer",
    )(
        tokens, pre_gain[None], q_norm_gain.reshape(-1, LANES), kv_norm_gain[None],
        post_gain[None], conv_taps, jnp.asarray(angles(nsp * rows)), *weights,
    )


def solution(mesh):
    placed = (
        P("sp", "tp"), P(), P(None, "tp"), P(None, "tp"), P(None, "tp"), P(None, "tp"), P(), P(),
        P(None, "tp"), P(), P(), P(), P(None, "tp"), P("tp", None), P("tp", None), P("tp"),
    )
    return jax.shard_map(
        functools.partial(body, mesh.shape["sp"], mesh.shape["tp"]),
        mesh=mesh,
        in_specs=placed,
        out_specs=(P("sp", "tp"), P("tp", "sp")),
        check_vma=False,
    )
```

```python
import functools
import math

import jax
import jax.numpy as jnp
import numpy as np
from jax import lax
from jax.experimental import pallas as pl
from jax.experimental.pallas import tpu as pltpu
from jax.sharding import PartitionSpec as P

NOPE = 64
ROPE = 32
VDIM = 64
TAPS = 3
LANES = 128
HALO = 16
TURN = 8
AHEAD = 2
WAVE = 3

EPSILON = 1e-06
THETA = 500000.0
NEGATIVE = -1e30
MESH = pl.DeviceIdType.MESH
BF = jnp.bfloat16
F32 = jnp.float32


def remote(src, dst, send, recv, **where):
    return pltpu.make_async_remote_copy(
        src_ref=src, dst_ref=dst, send_sem=send, recv_sem=recv, device_id=where, device_id_type=MESH
    )


def dot(a, b):
    return jnp.dot(a, b, preferred_element_type=F32)


def dot_nt(a, b):
    return lax.dot_general(a, b, (((1,), (1,)), ((), ())), preferred_element_type=F32)


def layer_kernel(
    nz, nx, n, chunk, heads,
    tok, pre_in, qg_in, kg_in, gain_in, taps_in, table, wo, wi, ws, wq, wk, wr, wu, wkv, wa, wc,
    out, logs,
    pre, qg, kg, gain, taps, buf, vo, vi, vs, vq, vk, vr, vu, vkv, va, vc, angle,
    vut, upk, upvt, qt, kvs, kn, turn, vt, sbuf, acc, top, low,
    near, near_square, near_k, near_r, near_q, near_c, far, factors, outer, ext, tail, halo, att,
    away, mine, pin, ysend, yin, peer, pown, total, sq, sqin,
    t_s, w_s, own_s, own_r, y_s, y_r, f_s, f_r,
    z_s, o_s, x_s, i_r, d_s, d_r, h_s, h_r,
    a_s, a_r, b_s, b_r, p_s, p_r, q_s, q_r,
):
    sp, tp = lax.axis_index("sp"), lax.axis_index("tp")
    nsp = nz * nx
    z, x = sp // nx, lax.rem(sp, nx)
    ny = n // 2
    y, core = tp // 2, lax.rem(tp, 2)
    partner = tp + 1 - 2 * core
    rows, width = tok.shape
    count = rows // chunk
    pairs = heads // 2
    rank = wkv.shape[0]
    factor2 = (NOPE + ROPE) ** (-0.5) * math.log2(math.e)
    side = pl.ds(pl.multiple_of(core * (rank // 2), LANES), rank // 2)

    def part(r):
        return pl.ds(r * chunk, chunk)

    tokens = [
        pltpu.make_async_copy(tok.at[part(r)], buf.at[tp, part(r)], t_s.at[r]) for r in range(count)
    ]
    place = pl.ds(pl.multiple_of(sp * rows, LANES), rows)
    pairs_of = (
        (wk, vk), (wr, vr), (wq, vq), (wi, vi), (ws, vs), (wo, vo), (wu, vu), (wkv, vkv),
        (table.at[:, place], angle), (qg_in, qg), (kg_in, kg), (pre_in, pre),
        (wa, va), (wc, vc), (gain_in, gain), (taps_in, taps),
    )
    loads = [pltpu.make_async_copy(a, b, w_s.at[i]) for i, (a, b) in enumerate(pairs_of)]
    for token in tokens:
        token.start()

    barrier = pltpu.get_barrier_semaphore()

    def greet(**where):
        pl.semaphore_signal(barrier, inc=1, device_id=where, device_id_type=MESH)

    for step in range(1, n):
        greet(tp=lax.rem(tp + step, n))
    for live, there in (
        (z > 0, sp - nx), (z < nz - 1, sp + nx), (sp > 0, sp - 1), (sp < nsp - 1, sp + 1)
    ):
        @pl.when(live)
        def _(there=there):
            greet(sp=there)

    for step in range(1, nx):
        greet(sp=z * nx + lax.rem(x + step, nx))
    heard = sum(
        jnp.where(live, 1, 0) for live in (z > 0, z < nz - 1, sp > 0, sp < nsp - 1)
    )
    loads[11].start()
    for load in loads[:11] + loads[12:]:
        load.start()
    with jax.named_scope("barrier"):
        pl.semaphore_wait(barrier, n - 1 + nx - 1 + heard)

    def y_copy(r, step):
        to = lax.rem(y + step, ny) * 2 + core
        here = buf.at[tp, part(r)]
        return remote(here, here, y_s.at[step - 1], y_r.at[r, step - 1], tp=to)

    def y_other(step):
        return lax.rem(y + ny - step, ny)

    def y_arrival(r, step):
        here = buf.at[y_other(step) * 2 + core, part(r)]
        return remote(here, here, y_s.at[step - 1], y_r.at[r, step - 1], tp=partner)

    def own_copy(r):
        here = buf.at[tp, part(r)]
        return remote(here, here, own_s.at[0], own_r.at[r], tp=partner)

    def own_arrival(r):
        here = buf.at[partner, part(r)]
        return remote(here, here, own_s.at[0], own_r.at[r], tp=partner)

    def forward(r, step):
        here = buf.at[y_other(step) * 2 + core, part(r)]
        return remote(here, here, f_s.at[step - 1], f_r.at[r, step - 1], tp=partner)

    def forward_arrival(r, step):
        here = buf.at[y_other(step) * 2 + 1 - core, part(r)]
        return remote(here, here, f_s.at[step - 1], f_r.at[r, step - 1], tp=partner)

    def tokens_sent():
        here = buf.at[tp]
        remote(here, here, own_s.at[0], own_r.at[0], tp=partner).wait_send()
        for step in range(1, ny):
            remote(here, here, y_s.at[step - 1], own_r.at[0], tp=partner).wait_send()
            remote(here, here, f_s.at[step - 1], own_r.at[0], tp=partner).wait_send()

    def piece(src, r):
        return kvs.at[src, r, :, side]

    def up_copy(k, r):
        src = sp - k * nx
        return remote(piece(src, r), piece(src, r), z_s.at[k], i_r.at[src, r], sp=sp + nx)

    def own_side(r, step):
        to = z * nx + lax.rem(x + step, nx)
        return remote(piece(sp, r), piece(sp, r), o_s.at[step - 1], i_r.at[sp, r], sp=to)

    def relay(k, r, step):
        src = sp - k * nx
        to = z * nx + lax.rem(x + step, nx)
        return remote(piece(src, r), piece(src, r), x_s.at[k - 1, step - 1], i_r.at[src, r], sp=to)

    def arrival(src, r):
        return remote(piece(src, r), piece(src, r), z_s.at[0], i_r.at[src, r], tp=partner)

    def share(src, r):
        return remote(piece(src, r), piece(src, r), d_s.at[src], d_r.at[src], tp=partner)

    def share_arrival(src):
        other = pl.ds(pl.multiple_of((1 - core) * (rank // 2), LANES), rank // 2)
        here = kvs.at[src, :, :, other]
        return remote(here, here, d_s.at[src], d_r.at[src], tp=partner)

    def block_sent(sem):
        here = kvs.at[sp, :, :, side]
        remote(here, here, sem, d_r.at[0], tp=partner).wait_send()

    def halo_copy():
        return remote(tail, halo, h_s.at[0], h_r.at[0], sp=sp + 1)

    with jax.named_scope("sendtok"):
        for r in range(count):
            tokens[r].wait()
            for step in range(1, ny):
                y_copy(r, step).start()
            own_copy(r).start()

    def lanes_of(other):
        return pl.ds(pl.multiple_of(other * 2 * width, LANES), 2 * width)

    def pick(other, here):
        return jnp.concatenate([buf[other * 2, here], buf[other * 2 + 1, here]], axis=1).astype(F32)

    def load_wait(start, stop):
        with jax.named_scope(f"wload{start}"):
            for load in loads[start:stop]:
                load.wait()

    qt[...] = jnp.zeros_like(qt)
    with jax.named_scope("ownwait"):
        for r in range(count):
            own_arrival(r).wait_recv()
    mine_here = lanes_of(y)
    load_wait(11, 12)
    wide = pick(y, pl.ds(0, rows))
    near_square[...] = jnp.broadcast_to(jnp.sum(wide * wide, axis=1, keepdims=True), (rows, LANES))
    near[...] = (wide * pre[:, mine_here]).astype(BF)
    load_wait(0, 2)
    near_k[...] = dot(near[...], vk[mine_here])
    near_r[...] = dot_nt(vr[:, mine_here], near[...])
    load_wait(2, 3)
    near_q[...] = dot(near[...], vq[mine_here])
    load_wait(3, 6)
    channels = vi.shape[1]
    for index, w in enumerate((vi, vs, vo)):
        near_c[:, index * channels : (index + 1) * channels] = dot(near[...], w[mine_here])

    load_wait(6, 11)
    with jax.named_scope("wturn"):
        vut[...] = vu[...].T
        for p in range(pairs):
            first, second = 2 * p * LANES, (2 * p + 1) * LANES
            upk[:, p * LANES : (p + 1) * LANES] = jnp.concatenate(
                [vkv[:, first : first + NOPE], vkv[:, second : second + NOPE]], axis=1
            )
        turned = vkv[...].T
        for h in range(heads):
            upvt[h * VDIM : (h + 1) * VDIM] = turned[h * LANES + NOPE : (h + 1) * LANES]

    def raise_keys(src, slot, span):
        here = pl.ds(span[0] * chunk, len(span) * chunk)

        def latent():
            return jnp.concatenate([kvs[src, r, :chunk] for r in span], axis=0)

        def keys(start, stop):
            kn[slot, here, start:stop] = dot(latent(), upk[:, start:stop]).astype(BF)

        def values():
            vt[slot, :, here] = dot_nt(upvt[...], latent()).astype(BF)

        def turns(r):
            packed = kvs[src, r, chunk:].astype(F32)
            tall = jnp.concatenate(
                [packed[:, g * LANES : (g + 1) * LANES] for g in range(ROPE // TURN)]
                + [jnp.zeros((LANES - ROPE, LANES), F32)],
                axis=0,
            )
            turn[slot, part(r)] = tall.T.astype(BF)

        wide = heads * NOPE
        cut = min(wide, 2 * LANES)
        parts = [functools.partial(keys, s, s + cut) for s in range(0, wide, cut)]
        return parts + [values] + [functools.partial(turns, r) for r in span]

    def do(parts):
        for one in parts:
            one()

    def units(todo, diagonal, parts=()):
        peaks, ready = {}, {}
        size = len(todo)

        def keys(c):
            return (c + 1) * chunk if diagonal else rows

        def score(i):
            c, p, slot = todo[i]
            k = keys(c)
            left = jnp.concatenate(
                [kn[slot, :k, p * LANES : (p + 1) * LANES], turn[slot, :k]], axis=1
            )
            s = dot(left, qt[c, p])
            if diagonal:
                last = s[k - chunk :]
                key = lax.broadcasted_iota(jnp.int32, last.shape, 0)
                query = lax.rem(lax.broadcasted_iota(jnp.int32, last.shape, 1), chunk)
                last = jnp.where(key <= query, last, NEGATIVE)
                s = last if k == chunk else jnp.concatenate([s[: k - chunk], last], axis=0)
            sbuf[i % (AHEAD + 2), :k] = s
            peaks[i] = jnp.max(s, axis=0, keepdims=True) * factor2

        def soften(i):
            c, p, slot = todo[i]
            peak = peaks.pop(i)
            shrink = None
            if not diagonal:
                before = top[c, p]
                peak = jnp.maximum(before, peak)
                shrink = jnp.exp2(before - peak)
            w = jnp.exp2(sbuf[i % (AHEAD + 2), : keys(c)] * factor2 - peak)
            sums = jnp.sum(w, axis=0, keepdims=True)
            low[c, p] = sums if diagonal else low[c, p] * shrink + sums
            top[c, p] = peak
            ready[i] = (w.astype(BF), shrink)

        def gather(i):
            c, p, slot = todo[i]
            w, shrink = ready.pop(i)
            o = dot(vt[slot, p * LANES : (p + 1) * LANES, : keys(c)], w)
            o = jnp.concatenate([o[:VDIM, :chunk], o[VDIM:, chunk:]], axis=1)
            acc[c, p] = o if diagonal else acc[c, p] * shrink + o

        parts = list(parts)
        for t in range(size + AHEAD + 1):
            if t < size:
                score(t)
            if parts:
                parts.pop(0)()
            if 0 <= t - AHEAD < size:
                soften(t - AHEAD)
            if 0 <= t - AHEAD - 1 < size:
                gather(t - AHEAD - 1)
        do(parts)

    items = z * nx + x

    def place_of(i):
        j = i - x - 1
        block, spot = (j + nx) // nx - 1, lax.rem(j + nx, nx)
        late = block >= z - 1
        column = jnp.where(late, False, spot == 0)
        step = jnp.where(late, spot + 1, spot)
        level = jnp.where(late, z, jnp.where(spot == 0, block + 2, block + 1))
        column = jnp.logical_or(j == -1, column)
        step = jnp.where(j == -1, 0, step)
        level = jnp.where(j == -1, 1, level)
        level = jnp.where(j < -1, 0, level)
        column = jnp.logical_and(j >= -1, column)
        across_x = jnp.where(j < -1, i, lax.rem(x + step, nx))
        return (z - level) * nx + across_x, column

    def pump(q, low=0):
        k, r = q // count + 1, q % count

        @pl.when(jnp.logical_and(k <= z, q >= low))
        def _():
            src = sp - k * nx
            arrival(src, r).wait_recv()

            @pl.when(z < nz - 1)
            def _():
                up_copy(k, r).start()

            for step in range(1, nx):
                relay(k, r, step).start()
            share(src, r).start()

    def fetch(i):
        src, column = place_of(i)

        @pl.when(jnp.logical_and(i < items, jnp.logical_not(column)))
        def _():
            for r in range(count):
                arrival(src, r).wait_recv()
                share(src, r).start()

    def shared(i):
        src, _ = place_of(i)
        with jax.named_scope("sharewait"):
            share_arrival(src).wait_recv()

    def prepare(i):
        with jax.named_scope("pump"):
            low = jnp.where(z < nz - 1, 6, 5)
            first = 5 + 2 * (i - jnp.minimum(x, 1))
            pump(first, low)
            pump(first + 1, low)
        with jax.named_scope("fetch"):
            fetch(i + 2)

    def pass_on(r):
        for step in range(1, ny):
            y_arrival(r, step).wait_recv()
            forward(r, step).start()

    def project(r):
        with jax.named_scope(f"tokwait{r}"):
            if r == 0:
                pass_on(r)
            for step in range(1, ny):
                forward_arrival(r, step).wait_recv()
        here = part(r)
        square = near_square[here, :1]
        for step in range(1, ny):
            wide = pick(y_other(step), here)
            square = square + jnp.sum(wide * wide, axis=1, keepdims=True)
            far[step - 1, here] = (wide * pre[:, lanes_of(y_other(step))]).astype(BF)
        factor = lax.rsqrt(square / (n * width) + EPSILON)
        factors[here] = jnp.broadcast_to(factor, (chunk, LANES))
        flat = jnp.broadcast_to(factor, (chunk, LANES)).T[:1]
        cosine, sine = angle[: ROPE // 2, here], angle[ROPE // 2 :, here]

        def rotate(first, second):
            return jnp.concatenate(
                [first * cosine - second * sine, second * cosine + first * sine], axis=0
            )

        kv, key, q = near_k[here], near_r[:, here], near_q[here]
        for step in range(1, ny):
            scaled, there = far[step - 1, here], lanes_of(y_other(step))
            kv = kv + dot(scaled, vk[there])
            key = key + dot_nt(vr[:, there], scaled)
        kv = kv * factor
        kv = kv * lax.rsqrt(jnp.mean(kv * kv, axis=1, keepdims=True) + EPSILON) * kg[...]
        kvs[sp, r, :chunk] = kv.astype(BF)
        key = key * flat
        key = rotate(key[: ROPE // 2], key[ROPE // 2 :])
        kvs[sp, r, chunk:] = jnp.concatenate(
            [key[g * TURN : (g + 1) * TURN] for g in range(ROPE // TURN)], axis=1
        ).astype(BF)
        @pl.when(z < nz - 1)
        def _():
            up_copy(0, r).start()

        for step in range(1, nx):
            @pl.when(x + step < nx)
            def _(step=step):
                own_side(r, step).start()

        for step in range(1, ny):
            q = q + dot(far[step - 1, here], vq[lanes_of(y_other(step))])
        q = q * factor
        gains = jnp.concatenate([qg[i : i + 1] for i in range(qg.shape[0])], axis=1)
        q = q * lax.rsqrt(jnp.mean(q * q, axis=1, keepdims=True) + EPSILON) * gains
        with jax.named_scope("passon"):
            if r + 1 < count:
                pass_on(r + 1)
            else:
                pump(0)
        query = dot_nt(vut[...], q.astype(BF))
        for h in range(heads):
            p, low_half = h // 2, h % 2
            base = h * (NOPE + ROPE)
            span = slice(low_half * chunk, (low_half + 1) * chunk)
            qt[r, p, low_half * NOPE : (low_half + 1) * NOPE, span] = query[
                base : base + NOPE
            ].astype(BF)
            middle = base + NOPE + ROPE // 2
            qt[r, p, 2 * NOPE : 2 * NOPE + ROPE, span] = rotate(
                query[base + NOPE : middle], query[middle : base + NOPE + ROPE]
            ).astype(BF)

    def branch(r):
        here = part(r)
        factor = factors[here, :1]

        def gate(index, w):
            value = near_c[here, index * channels : (index + 1) * channels]
            for step in range(1, ny):
                value = value + dot(far[step - 1, here], w[lanes_of(y_other(step))])
            return (value * factor).astype(BF)

        inner = gate(0, vi).astype(F32)
        source = gate(1, vs).astype(F32)
        driven = (inner * source).astype(BF)
        ext[8 + r * chunk : 8 + (r + 1) * chunk] = driven.astype(F32)
        if r == count - 1:
            tail[...] = driven[chunk - HALO :]

            @pl.when(sp < nsp - 1)
            def _():
                halo_copy().start()
        outer[here] = gate(2, vo)

    for r in range(count):
        project(r)
    with jax.named_scope("pump1"):
        pump(1)
    for r in range(count - 1, -1, -1):
        with jax.named_scope("branch"):
            branch(r)
    with jax.named_scope("diag"):
        do(raise_keys(sp, 0, list(range(count))))
        units([(r, p, 0) for r in range(count - 1) for p in range(pairs)], True)
    with jax.named_scope("prefetch"):
        fetch(0)
        fetch(1)
        pump(2)
        pump(3)
    with jax.named_scope("diag"):
        units([(count - 1, p, 0) for p in range(pairs)], True)
    with jax.named_scope("pump4"):
        pump(4)

        @pl.when(z < nz - 1)
        def _():
            pump(5)

    everything = list(range(count))
    many = items >= WAVE

    @pl.when(many)
    def _():
        shared(0)
        with jax.named_scope("raise0"):
            do(raise_keys(place_of(0)[0], 0, everything))

        def whole(i, carry):
            prepare(i)
            shared(i + 1)
            with jax.named_scope("units"):
                units(
                    [(c, p, 0) for c in everything for p in range(pairs)], False,
                    raise_keys(place_of(i + 1)[0], 1, everything),
                )
                for old in (kn, vt, turn):
                    old[0] = old[1]
            return carry

        peel = jnp.logical_and(x == 0, items > WAVE)

        @pl.when(peel)
        def _():
            with jax.named_scope("units"):
                units([(c, p, 0) for c in everything for p in range(pairs)], False)
            prepare(0)
            shared(1)
            do(raise_keys(place_of(1)[0], 0, everything))

        lax.fori_loop(jnp.where(peel, 1, 0), items - WAVE, whole, 0)
        for w in range(WAVE - 1):
            prepare(items - WAVE + w)
            shared(items - WAVE + w + 1)
            with jax.named_scope("waveunits"):
                units(
                    [(0, p, w) for p in range(pairs)], False,
                    raise_keys(place_of(items - WAVE + w + 1)[0], w + 1, everything),
                )
        with jax.named_scope("waveunits"):
            units([(0, p, WAVE - 1) for p in range(pairs)], False)

    @pl.when(jnp.logical_not(many))
    def _():
        def ready(w, carry):
            prepare(w)
            shared(w)
            do(raise_keys(place_of(w)[0], w, everything))
            return carry

        lax.fori_loop(0, items, ready, 0)

    @pl.when(sp == 0)
    def _():
        ext[:8] = jnp.zeros((8, ext.shape[1]), F32)

    @pl.when(sp > 0)
    def _():
        remote(tail, halo, h_s.at[0], h_r.at[0], tp=partner).wait_recv()
        ext[:8] = halo[...].astype(F32)[HALO - 8 :]

    def product(r, dest):
        columns = pl.ds(pl.multiple_of(dest * width, width), width)
        return (
            dot(att[part(r), : heads * VDIM], va[:, columns])
            + dot(att[part(r), heads * VDIM :], vc[:, columns])
        ).astype(BF)

    def to_partner(r, step):
        return remote(
            away.at[step, part(r)], pin.at[step, part(r)], a_s.at[step - 1], a_r.at[r, step - 1], tp=partner
        )

    def across(r, step):
        to = lax.rem(y + step, ny) * 2 + core
        return remote(
            ysend.at[step, part(r)], yin.at[step, part(r)], b_s.at[step - 1], b_r.at[r, step - 1], tp=to
        )

    def home(r):
        return remote(peer.at[part(r)], pown.at[part(r)], p_s.at[0], p_r.at[r], tp=partner)

    def squares(r, step):
        return remote(
            sq.at[r], sqin.at[step, r], q_s.at[step - 1], q_r.at[r, step - 1], tp=lax.rem(tp + step, n)
        )

    for load in loads[12:]:
        load.wait()

    def send_on(c):
        for step in range(1, ny):
            with jax.named_scope("partnerwait"):
                to_partner(c, step).wait_recv()
            ysend[step, part(c)] = (
                mine[step, part(c)].astype(F32) + pin[step, part(c)].astype(F32)
            ).astype(BF)
            across(c, step).start()

    for c in range(count):
        if c > 0:
            @pl.when(many)
            def _(c=c):
                with jax.named_scope("lastunits"):
                    units([(c, p, w) for w in range(WAVE) for p in range(pairs)], False)

        @pl.when(jnp.logical_not(many))
        def _(c=c):
            def last(w, carry):
                units([(c, p, w) for p in range(pairs)], False)
                return carry

            lax.fori_loop(0, items, last, 0)

        for p in range(pairs):
            value = acc[c, p] / low[c, p]
            both = jnp.concatenate([value[:, :chunk], value[:, chunk:]], axis=0)
            att[part(c), p * LANES : (p + 1) * LANES] = both.T.astype(BF)
            log = top[c, p] * math.log(2.0) + jnp.log(low[c, p])
            logs[2 * p : 2 * p + 1, part(c)] = log[:, :chunk]
            logs[2 * p + 1 : 2 * p + 2, part(c)] = log[:, chunk:]
        conv = jnp.zeros((chunk, ext.shape[1]), F32)
        for index in range(TAPS):
            start = 8 + c * chunk - (TAPS - 1) + index
            conv = conv + taps[index : index + 1].astype(F32) * ext[start : start + chunk]
        att[part(c), heads * VDIM :] = (outer[part(c)].astype(F32) * conv).astype(BF)
        for step in range(1, ny):
            dest = lax.rem(y + step, ny) * 2
            away[step, part(c)] = product(c, dest + 1 - core)
            to_partner(c, step).start()
            mine[step, part(c)] = product(c, dest + core)
        peer[part(c)] = product(c, partner)
        home(c).start()
        total[part(c)] = product(c, tp).astype(F32)
        send_on(c)
    tokens_sent()
    for step in range(1, nx):
        @pl.when(x + step < nx)
        def _(step=step):
            block_sent(o_s.at[step - 1])

    @pl.when(sp < nsp - 1)
    def _():
        halo_copy().wait_send()

    def sent(i, carry):
        block_sent(d_s.at[place_of(i)[0]])
        return carry

    lax.fori_loop(0, items, sent, 0)

    def relayed(k, carry):
        for step in range(1, nx):
            block_sent(x_s.at[k - 1, step - 1])
        return carry

    lax.fori_loop(1, z + 1, relayed, 0)

    @pl.when(z < nz - 1)
    def _():
        def raised(k, carry):
            block_sent(z_s.at[k])
            return carry

        lax.fori_loop(0, z + 1, raised, 0)

    for r in range(count):
        with jax.named_scope("homewait"):
            home(r).wait_recv()
        value = total[part(r)] + pown[part(r)].astype(F32)
        for step in range(1, ny):
            with jax.named_scope("acrosswait"):
                across(r, step).wait_recv()
            value = value + yin[step, part(r)].astype(F32)
        total[part(r)] = value
        sums = jnp.sum(value * value, axis=1, keepdims=True)
        sq[r] = jnp.broadcast_to(sums, (chunk, LANES)).T[:8]
        for step in range(1, n):
            squares(r, step).start()
    for r in range(count):
        whole_sum = sq[r]
        for step in range(1, n):
            with jax.named_scope("sqwait"):
                squares(r, step).wait_recv()
            whole_sum = whole_sum + sqin[step, r]
        with jax.named_scope("outs"):
          scale = lax.rsqrt(whole_sum / (n * width) + EPSILON)
          column = jnp.broadcast_to(scale[:1], (LANES, chunk)).T[:, :1]
          out[part(r)] = (total[part(r)] * column * gain[...]).astype(BF)

    remote(peer, pown, p_s.at[0], p_r.at[0], tp=partner).wait_send()
    for step in range(1, ny):
        remote(peer, pown, a_s.at[step - 1], p_r.at[0], tp=partner).wait_send()
        remote(peer, pown, b_s.at[step - 1], p_r.at[0], tp=partner).wait_send()
    for step in range(1, n):
        remote(sq, sqin.at[step], q_s.at[step - 1], p_r.at[0], tp=partner).wait_send()


DMA = pltpu.SemaphoreType.DMA


def angles(tokens):
    freqs = np.float32(THETA) ** (-np.arange(0, ROPE, 2, dtype=np.float32) / np.float32(ROPE))
    phase = freqs.astype(np.float32)[:, None] * np.arange(tokens, dtype=np.float32)[None, :]
    phase = phase.astype(np.float64)
    return np.concatenate([np.cos(phase), np.sin(phase)], axis=0).astype(np.float32)


def body(
    nsp, ntp,
    tokens, pre_gain, outer_gate_weight, inner_gate_weight, source_weight, conv_taps,
    q_down_weight, q_norm_gain, q_up_weight, kv_down_weight, rope_key_weight, kv_norm_gain,
    kv_up_weight, attn_out_weight, conv_out_weight, post_gain,
):
    rows, width = tokens.shape
    ny = ntp // 2
    nx = ny if nsp % ny == 0 else 1
    nz = nsp // nx
    chunk = LANES
    count = rows // chunk
    q_rank, rank = q_down_weight.shape[1], kv_down_weight.shape[1]
    channels = outer_gate_weight.shape[1]
    heads = q_up_weight.shape[1] // (NOPE + ROPE)
    pairs = heads // 2
    struct = jax.ShapeDtypeStruct
    v = pltpu.VMEM
    whole = pl.BlockSpec(memory_space=pltpu.VMEM)
    anywhere = pl.BlockSpec(memory_space=pl.ANY)
    rope_turned = rope_key_weight.T
    weights = (
        outer_gate_weight, inner_gate_weight, source_weight, q_down_weight, kv_down_weight,
        rope_turned, q_up_weight, kv_up_weight, attn_out_weight, conv_out_weight,
    )
    small = (
        pre_gain[None], q_norm_gain.reshape(-1, LANES), kv_norm_gain[None], post_gain[None], conv_taps,
    )
    block = (ny, rows, width)
    return pl.pallas_call(
        functools.partial(layer_kernel, nz, nx, ntp, chunk, heads),
        out_shape=[v((rows, width), BF), v((heads, rows), F32)],
        in_specs=[anywhere] * (7 + len(weights)),
        out_specs=[whole] * 2,
        scratch_shapes=[v(w.shape, w.dtype) for w in small]
        + [v((ntp, rows, width), BF)]
        + [v(w.shape, BF) for w in weights]
        + [
            v((ROPE, rows), F32),
            v(q_up_weight.shape[::-1], BF),
            v((rank, heads * NOPE), BF), v((heads * VDIM, rank), BF),
            v((count, pairs, 2 * LANES, 2 * chunk), BF),
            v((nsp, count, chunk + TURN, rank), BF),
            v((WAVE, rows, heads * NOPE), BF), v((WAVE, rows, LANES), BF),
            v((WAVE, heads * VDIM, rows), BF),
            v((AHEAD + 2, rows, 2 * chunk), F32),
            v((count, pairs, VDIM, 2 * chunk), F32),
            v((count, pairs, 1, 2 * chunk), F32), v((count, pairs, 1, 2 * chunk), F32),
            v((rows, 2 * width), BF), v((rows, LANES), F32), v((rows, rank), F32),
            v((ROPE, rows), F32), v((rows, q_rank), F32), v((rows, 3 * channels), F32),
            v((ny - 1, rows, 2 * width), BF), v((rows, LANES), F32),
            v((rows, channels), BF), v((8 + rows, channels), F32),
            v((HALO, channels), BF), v((HALO, channels), BF),
            v((rows, heads * VDIM + channels), BF),
        ]
        + [v(block, BF)] * 5
        + [
            v((rows, width), BF), v((rows, width), BF), v((rows, width), F32),
            v((count, 8, chunk), F32), v((ntp, count, 8, chunk), F32),
            DMA((count,)), DMA((16,)), DMA((1,)), DMA((count,)),
            DMA((ny - 1,)), DMA((count, ny - 1)), DMA((ny - 1,)), DMA((count, ny - 1)),
            DMA((nz,)), DMA((nx - 1,)), DMA((nz - 1, nx - 1)),
            DMA((nsp, count)), DMA((nsp,)), DMA((nsp,)), DMA((1,)), DMA((1,)),
            DMA((ny - 1,)), DMA((count, ny - 1)), DMA((ny - 1,)), DMA((count, ny - 1)),
            DMA((1,)), DMA((count,)), DMA((ntp - 1,)), DMA((count, ntp - 1)),
        ],
        compiler_params=pltpu.CompilerParams(
            collective_id=0, has_side_effects=True, vmem_limit_bytes=60 * 1024 * 1024
        ),
        name="layer",
    )(
        tokens, *small, jnp.asarray(angles(nsp * rows)), *weights,
    )


def solution(mesh):
    placed = (
        P("sp", "tp"), P(), P(None, "tp"), P(None, "tp"), P(None, "tp"), P(None, "tp"), P(), P(),
        P(None, "tp"), P(), P(), P(), P(None, "tp"), P("tp", None), P("tp", None), P("tp"),
    )
    return jax.shard_map(
        functools.partial(body, mesh.shape["sp"], mesh.shape["tp"]),
        mesh=mesh,
        in_specs=placed,
        out_specs=(P("sp", "tp"), P("tp", "sp")),
        check_vma=False,
    )
```
